512 devices in a mesh: sp: 32 (over z, x), dp: 16 (over y, core).
Axes of the slice: x: 4, y: 8, z: 8, core: 2. Of those that a mesh axis runs over, the one named last changes fastest.
Arguments:
- tokens: bfloat16 [128, 2048, 2048], P('dp', 'sp'), may hold values from -6 to 6
- pre_gain: float32 [2048], replicated, may hold values from 0.1 to 1.9
- w_query: bfloat16 [2048, 512], P('dp'), may hold values from -0.125 to 0.125
- w_forget: bfloat16 [2048, 512], P('dp'), may hold values from -0.125 to 0.125
- w_value: bfloat16 [2048, 512], P('dp'), may hold values from -0.125 to 0.125
- w_gate: bfloat16 [2048, 512], P('dp'), may hold values from -0.125 to 0.125
- lower_bound: float32 [512], replicated, may hold values from 0.8 to 1
- extra_decay: float32 [512, 2048], P(('dp', 'sp')), may hold values from -1.5 to 0
- initial_state: float32 [512, 128, 128], P(('dp', 'sp')), may hold values from -0.18 to 0.18
- norm_gain: float32 [128], replicated, may hold values from 0.1 to 1.9
- w_out: bfloat16 [512, 2048], P('dp'), may hold values from -0.25 to 0.25
- post_gain: float32 [2048], replicated, may hold values from 0.1 to 1.9
Outputs:
- layer_out: bfloat16 [128, 2048, 2048], P('dp', 'sp')
The draws below stay inside these ranges and needn't reach their ends.
All inputs are finite; a program needn't handle non-finite values.
Results may differ from the reference program's by a relative error of at most 0.015.
Values may be sent and summed in bfloat16 or wider, within the bound.
No kernel may reach another device: no remote copies, remote signals or barrier semaphores. Data moves between devices by JAX's collectives and lax.ppermute only.
A program may use at most 64 MiB of HBM per device.

```python
import math
import jax
import jax.numpy as jnp
from jax import lax

D = 2048
HEADS = 4
HK = 128
HV = 128
BLOCK = 64
LOC = 64
SEQUENCE_LENGTH = 2048
SEQS = 128


def draw_lower_bound(key, part):
    key_rows = jax.random.split(jax.random.fold_in(key, 11), 4)
    order = jax.random.permutation(key_rows[0], HEADS)
    fast_count = HEADS // 2
    fast_heads = order < fast_count
    slow_gap = jax.random.uniform(key_rows[1], (HEADS, 1), jnp.float32, 0.1, 0.5) / SEQUENCE_LENGTH
    fast_gap = jnp.exp(jax.random.uniform(key_rows[2], (HEADS, 1), jnp.float32, math.log(1.0 / 40.0), math.log(1.0 / 15.0)))
    spread = jnp.exp(jax.random.uniform(key_rows[3], (HEADS, HK), jnp.float32, math.log(0.5), math.log(2.0)))
    forget_gap = jnp.where(fast_heads[:, None], fast_gap, slow_gap) * spread
    return (1.0 - forget_gap).reshape(HEADS * HK)


def draw_extra_decay(key, part):
    key_rows = jax.random.split(jax.random.fold_in(key, 23), 3)
    count_of_rows = SEQS * HEADS
    block_count = SEQUENCE_LENGTH // LOC
    rate_low = 0.3
    rates = jnp.exp(jax.random.uniform(key_rows[0], (count_of_rows, block_count), jnp.float32, math.log(rate_low), math.log(1.2))) / SEQUENCE_LENGTH
    base_offset = -jnp.repeat(rates, LOC, axis=1)
    spike_position = jax.random.randint(key_rows[1], (count_of_rows, 2), 0, SEQUENCE_LENGTH)
    spike_fraction = jax.random.uniform(key_rows[2], (count_of_rows, 2), jnp.float32, 0.2, 0.5)
    token_position = jnp.arange(SEQUENCE_LENGTH, dtype=jnp.int32)
    match_count = token_position[None, None, :] == spike_position[:, :, None]
    spike_events = jnp.sum(jnp.where(match_count, jnp.log1p(-spike_fraction)[:, :, None], 0.0), axis=1)
    return base_offset + spike_events


def block_levels(own_key, extent, cuts, low, largest):
    factor_of, own = 1.0, jax.random.fold_in(own_key, 6)
    for position, parts in cuts:
        draws = jnp.exp(jax.random.uniform(jax.random.fold_in(own, position), (parts,), jnp.float32, low / len(cuts), largest / len(cuts)))
        factor_of = factor_of * jnp.repeat(draws, extent[position] // parts).reshape([-1 if axis == position else 1 for axis in range(len(extent))])
    return factor_of


def scatter_about(key, dims, width, bound, cuts=(), held_as=jnp.bfloat16):
    level = block_levels(key, dims, cuts, -0.22, 0.18) if cuts else 1.0
    entries = jax.random.normal(key, dims, jnp.float32) * width * level
    return jnp.minimum(jnp.maximum(entries, -bound), bound).astype(held_as)


def setup_inputs(seed: int = 0) -> dict:
    key_of = jax.random.split(jax.random.key(seed), 13)
    return {
        "tokens": scatter_about(key_of[0], (SEQS, SEQUENCE_LENGTH, D), 1.0, 6.0, ((0, 16), (1, 32))),
        "pre_gain": jnp.clip(1.0 + 0.18 * jax.random.normal(key_of[1], (D,), jnp.float32), 0.1, 1.9),
        "w_query": scatter_about(key_of[2], (D, HEADS * HK), D ** -0.5, 0.125, ((0, 16),)),
        "w_forget": scatter_about(key_of[3], (D, HEADS * HK), D ** -0.5, 0.125, ((0, 16),)),
        "w_value": scatter_about(key_of[4], (D, HEADS * HV), D ** -0.5, 0.125, ((0, 16),)),
        "w_gate": scatter_about(key_of[5], (D, HEADS * HV), D ** -0.5, 0.125, ((0, 16),)),
        "lower_bound": draw_lower_bound(jax.random.fold_in(key_of[12], 71), 0),
        "extra_decay": draw_extra_decay(jax.random.fold_in(key_of[12], 71), 0),
        "initial_state": scatter_about(key_of[8], (SEQS * HEADS, HK, HV), 0.03, 0.18, ((0, 512),), jnp.float32),
        "norm_gain": jnp.clip(1.0 + 0.18 * jax.random.normal(key_of[9], (HV,), jnp.float32), 0.1, 1.9),
        "w_out": scatter_about(key_of[10], (HEADS * HV, D), (HEADS * HV) ** -0.5, 0.25, ((0, 16),)),
        "post_gain": jnp.clip(1.0 + 0.18 * jax.random.normal(key_of[11], (D,), jnp.float32), 0.1, 1.9),
    }


EPS = 1e-06

def rms_scale(matrix, gain):
    widened = matrix.astype(jnp.float32)
    return widened * lax.rsqrt(lax.optimization_barrier(jnp.mean(widened * widened, axis=-1, keepdims=True)) + EPS) * gain

def recur_item(queries, keys_in, values, log_decay, state_zero):
    length = queries.shape[0]
    block_count = length // BLOCK

    def blocks(matrix):
        return matrix.reshape(block_count, BLOCK, matrix.shape[-1])
    causal_mask = jnp.tril(jnp.ones((BLOCK, BLOCK), dtype=bool))[:, :, None]

    def block_step(carried_state, inputs):
        query_block, key_block, value_block, decay_block = inputs
        cumulative = jnp.cumsum(decay_block, axis=0)
        carried = jnp.dot(query_block * jnp.exp(cumulative), carried_state, precision=lax.Precision.HIGHEST)
        log_gaps = cumulative[:, None, :] - cumulative[None, :, :]
        decay_weight = jnp.where(causal_mask, jnp.exp(jnp.minimum(log_gaps, 0.0)), 0.0)
        scores = jnp.einsum('tk,sk,tsk->ts', query_block, key_block, decay_weight, precision=lax.Precision.HIGHEST)
        within = jnp.dot(scores, value_block, precision=lax.Precision.HIGHEST)
        block_end = cumulative[-1]
        added_state = jnp.dot((key_block * jnp.exp(block_end[None, :] - cumulative)).T, value_block, precision=lax.Precision.HIGHEST)
        return (jnp.exp(block_end)[:, None] * carried_state + added_state, carried + within)
    _, block_outs = lax.scan(block_step, state_zero, (blocks(queries), blocks(keys_in), blocks(values), blocks(log_decay)))
    return block_outs.reshape(length, values.shape[-1])

def reference(tokens, pre_gain, w_query, w_forget, w_value, w_gate, lower_bound, extra_decay, initial_state, norm_gain, w_out, post_gain):
    forget_gap = (1.0 - lower_bound).reshape(HEADS, HK)
    states = initial_state.reshape(SEQS, HEADS, HK, HV)
    extras = extra_decay.reshape(SEQS, HEADS, SEQUENCE_LENGTH)
    query_weight = w_query.reshape(D, HEADS, HK).astype(jnp.float32)
    forget_weight = w_forget.reshape(D, HEADS, HK).astype(jnp.float32)
    value_weight = w_value.reshape(D, HEADS, HV).astype(jnp.float32)
    gate_weight = w_gate.reshape(D, HEADS, HV).astype(jnp.float32)
    out_weight = w_out.reshape(HEADS, HV, D).astype(jnp.float32)

    def one_sequence(inputs):
        row_block, state_zero, extra_rows = inputs
        norm_result = rms_scale(row_block, pre_gain).astype(jnp.bfloat16).astype(jnp.float32)
        q_pre = jnp.einsum('ld,dhk->hlk', norm_result, query_weight).astype(jnp.bfloat16)
        f_pre = jnp.einsum('ld,dhk->hlk', norm_result, forget_weight).astype(jnp.bfloat16)
        v_pre = jnp.einsum('ld,dhk->hlk', norm_result, value_weight).astype(jnp.bfloat16)
        g_pre = jnp.einsum('ld,dhk->hlk', norm_result, gate_weight).astype(jnp.bfloat16)
        queries = jax.nn.silu(q_pre.astype(jnp.float32))
        keys_in = forget_gap[:, None, :] * jax.nn.sigmoid(-f_pre.astype(jnp.float32))
        log_decay = jnp.log1p(-keys_in) + extra_rows[:, :, None]
        values = v_pre.astype(jnp.float32)
        outputs = jax.vmap(recur_item)(queries, keys_in, values, log_decay, state_zero)
        head_normed = (outputs * lax.rsqrt(lax.optimization_barrier(jnp.mean(outputs * outputs, axis=-1, keepdims=True)) + EPS) * norm_gain).astype(jnp.bfloat16)
        head_normed = lax.optimization_barrier(head_normed)
        gated = (head_normed.astype(jnp.float32) * jax.nn.silu(g_pre.astype(jnp.float32))).astype(jnp.bfloat16)
        mixed = jnp.einsum('hlv,hvd->ld', gated.astype(jnp.float32), out_weight)
        return rms_scale(mixed, post_gain).astype(jnp.bfloat16)
    return lax.map(one_sequence, (tokens, states, extras))
```

```python
import functools

import jax
import jax.numpy as jnp
from jax import lax
from jax.experimental import pallas as pl
from jax.experimental.pallas import tpu as pltpu
from jax.sharding import Mesh
from jax.sharding import PartitionSpec as P

HEADS = 4
HK = 128
HV = 128
CHUNK = 128
SP = ("z", "x")
DP = ("y", "c")
DP_SP = ("y", "c", "z", "x")
OFFSETS = (0, -1, 1, -2, 2, -3, 3, 4)
ROWS = 128
OUT_ROWS = 32
EPS = 1e-06


F32 = jnp.float32
BF16 = jnp.bfloat16


def shifted(a, step):
    size = lax.axis_size("y")
    return lax.ppermute(a, "y", [(i, (i + step) % size) for i in range(size)])


def swapped(a):
    return lax.ppermute(a, "c", [(0, 1), (1, 0)])


def gathered_y(shard):
    pieces = [shard]
    up = down = shard
    for _ in range(3):
        up, down = shifted(up, 1), shifted(down, -1)
        pieces += [up, down]
    half = shard.shape[0] // 2
    pieces += [shifted(up[:half], 1), shifted(down[half:], -1)]
    return jnp.concatenate(pieces, axis=0)


def dot(a, b):
    return jnp.dot(a, b, preferred_element_type=F32)


def dot_nt(a, b):
    return lax.dot_general(a, b, (((1,), (1,)), ((), ())), preferred_element_type=F32)


def dot_tn(a, b):
    return lax.dot_general(a, b, (((0,), (0,)), ((), ())), preferred_element_type=F32)


def sigmoid(a):
    return 0.5 * jnp.tanh(0.5 * a) + 0.5


def place(where_ref, j):
    core = where_ref[1] if j < len(OFFSETS) else 1 - where_ref[1]
    return 2 * ((where_ref[0] + OFFSETS[j % len(OFFSETS)] + 8) & 7) + core


def norm_kernel(where_ref, x_ref, gain_ref, out_ref):
    x = x_ref[...].astype(F32)
    scale = lax.rsqrt(jnp.mean(x * x, axis=-1, keepdims=True) + EPS)
    for j in range(2 * len(OFFSETS)):
        start = pl.multiple_of(place(where_ref, j) * ROWS, ROWS)
        part = x_ref[:, pl.ds(start, ROWS)].astype(F32) * scale * gain_ref[:, pl.ds(start, ROWS)]
        out_ref[:, j * ROWS : (j + 1) * ROWS] = part.astype(BF16)


def normed_tokens(tokens, pre_gain, where):
    rows, width = tokens.shape
    tile = 128
    return pl.pallas_call(
        norm_kernel,
        grid_spec=pltpu.PrefetchScalarGridSpec(
            num_scalar_prefetch=1,
            grid=(rows // tile,),
            in_specs=[
                pl.BlockSpec((tile, width), lambda i, b: (i, 0)),
                pl.BlockSpec((1, width), lambda i, b: (0, 0)),
            ],
            out_specs=pl.BlockSpec((tile, width), lambda i, b: (i, 0)),
        ),
        out_shape=jax.ShapeDtypeStruct((rows, width), BF16),
        name="norm",
    )(where, tokens, pre_gain.reshape(1, width))


def project_kernel(a_ref, own_ref, other_ref, out_ref):
    half = own_ref.shape[0]
    total = dot(a_ref[:, :half], own_ref[...]) + dot(a_ref[:, half:], other_ref[...])
    out_ref[...] = total.astype(BF16).reshape(out_ref.shape)


def project_heads(normed, own, other, seqs, local_len):
    wide = own.shape[1] // HEADS
    half = own.shape[0]
    return pl.pallas_call(
        project_kernel,
        grid=(HEADS,),
        in_specs=[
            pl.BlockSpec(normed.shape, lambda h: (0, 0)),
            pl.BlockSpec((half, wide), lambda h: (0, h)),
            pl.BlockSpec((half, wide), lambda h: (0, h)),
        ],
        out_specs=pl.BlockSpec((seqs, 1, local_len, wide), lambda h: (0, h, 0, 0)),
        out_shape=jax.ShapeDtypeStruct((seqs, HEADS, local_len, wide), BF16),
        name="project",
    )(normed, own, other)


def recur_kernel(qfv_ref, run_ref, gap_ref, state_ref, gain_ref, out_ref):
    length = qfv_ref.shape[0]
    row = lax.broadcasted_iota(jnp.int32, (CHUNK, CHUNK), 0)
    col = lax.broadcasted_iota(jnp.int32, (CHUNK, CHUNK), 1)
    causal = row >= col
    ones = causal.astype(F32).astype(BF16)
    gap = gap_ref[...]
    gain = gain_ref[...]

    def step(b, state):
        rows = pl.ds(pl.multiple_of(b * CHUNK, CHUNK), CHUNK)
        q = qfv_ref[rows, 0:HK].astype(F32)
        f = qfv_ref[rows, HK : 2 * HK].astype(F32)
        v = qfv_ref[rows, 2 * HK :]
        queries = q * sigmoid(q)
        keys = gap * sigmoid(-f)
        decay = jnp.log1p(-keys)
        high = decay.astype(BF16)
        low = (decay - high.astype(F32)).astype(BF16)
        total = dot(ones, high) + dot(ones, low)
        run_row = run_ref[pl.ds(b, 1), :]
        run_rows = jnp.broadcast_to(run_row, (CHUNK, CHUNK))
        run_cols = run_rows.T
        q_scaled = queries * jnp.exp(total)
        k_scaled = keys * jnp.exp(-total)
        scores = dot_nt(q_scaled.astype(BF16), k_scaled.astype(BF16))
        weight = jnp.exp(jnp.minimum(run_cols - run_rows, 0.0))
        scores = jnp.where(causal, scores * weight, 0.0).astype(BF16)
        carried = (q_scaled * jnp.exp(run_cols)).astype(BF16)
        out = dot(scores, v) + dot_nt(carried, state.astype(BF16))
        end = total[CHUNK - 1 :, :]
        run_end = run_cols[CHUNK - 1 :, :]
        k_end = k_scaled * jnp.exp(end) * jnp.exp(run_end - run_cols)
        added = dot_tn(v, k_end.astype(BF16))
        scale = lax.rsqrt(jnp.mean(out * out, axis=-1, keepdims=True) + EPS)
        out_ref[rows, :] = (out * scale * gain).astype(BF16)
        return state * jnp.exp(end + run_end) + added

    lax.fori_loop(0, length // CHUNK, step, state_ref[...], unroll=2)


def recurred(qfv, run, gap, state, gain):
    return pl.pallas_call(
        recur_kernel,
        out_shape=jax.ShapeDtypeStruct((qfv.shape[0], HV), BF16),
        name="recur",
    )(qfv, run, gap, state, gain)


def gate_kernel(where_ref, a_ref, own_ref, other_ref, gate_ref, weight_ref):
    half = own_ref.shape[0]
    wide = HEADS * HV
    total = dot(a_ref[:, :half], own_ref[:, :wide]) + dot(a_ref[:, half:], other_ref[:, :wide])
    gate = total.astype(BF16).astype(F32)
    gate_ref[...] = gate * sigmoid(gate)
    for k, stack in enumerate((own_ref, other_ref)):
        for j in range(len(OFFSETS)):
            start = pl.multiple_of(place(where_ref, k * len(OFFSETS) + j) * OUT_ROWS, OUT_ROWS)
            for n in range(ROWS // OUT_ROWS):
                first = j * ROWS + n * OUT_ROWS
                weight_ref[pl.ds(start, OUT_ROWS), n * wide : (n + 1) * wide] = stack[
                    first : first + OUT_ROWS, wide:
                ]


def gate_and_weight(where, normed, own, other, width):
    rows = normed.shape[0]
    wide = HEADS * HV
    vmem = pl.BlockSpec(memory_space=pltpu.VMEM)
    return pl.pallas_call(
        gate_kernel,
        in_specs=[pl.BlockSpec(memory_space=pltpu.SMEM), vmem, vmem, vmem],
        out_specs=(vmem, vmem),
        out_shape=(
            jax.ShapeDtypeStruct((rows, wide), F32),
            jax.ShapeDtypeStruct((wide, width), BF16),
        ),
        name="gate",
    )(where, normed, own, other)


def output_kernel(heads_ref, gate_ref, weight_ref, gain_ref, out_ref):
    seqs, _, local_len, _ = heads_ref.shape
    gated = []
    for h in range(HEADS):
        head = heads_ref[:, h].reshape(seqs * local_len, HV).astype(F32)
        gated.append((head * gate_ref[:, h * HV : (h + 1) * HV]).astype(BF16))
    mixed = dot(jnp.concatenate(gated, axis=1), weight_ref[...])
    scale = lax.rsqrt(jnp.mean(mixed * mixed, axis=-1, keepdims=True) + EPS)
    out_ref[...] = (mixed * scale * gain_ref[...]).astype(BF16).reshape(out_ref.shape)


def output_rows(heads, gate, weight, post_gain):
    seqs, _, local_len, _ = heads.shape
    width = weight.shape[1]
    wide = HEADS * HV
    group = 2
    return pl.pallas_call(
        output_kernel,
        grid=(seqs // group,),
        in_specs=[
            pl.BlockSpec((group, HEADS, local_len, HV), lambda i: (i, 0, 0, 0)),
            pl.BlockSpec((group * local_len, wide), lambda i: (i, 0)),
            pl.BlockSpec((wide, width), lambda i: (0, 0)),
            pl.BlockSpec((1, width), lambda i: (0, 0)),
        ],
        out_specs=pl.BlockSpec((group, local_len, width), lambda i: (i, 0, 0)),
        out_shape=jax.ShapeDtypeStruct((seqs, local_len, width), BF16),
        name="output",
    )(heads, gate, weight, post_gain.reshape(1, width))


def body(
    tokens,
    pre_gain,
    w_query,
    w_forget,
    w_value,
    w_gate,
    lower_bound,
    extra_decay,
    initial_state,
    norm_gain,
    w_out,
    post_gain,
):
    seqs, local_len, width = tokens.shape
    y, c = lax.axis_index("y"), lax.axis_index("c")
    where = jnp.stack([y, c]).astype(jnp.int32)

    by_head = [w.reshape(ROWS, HEADS, HK) for w in (w_query, w_forget, w_value)]
    first = jnp.concatenate(by_head, axis=2).reshape(ROWS, HEADS * 3 * HK)
    wide = HEADS * HV
    stacked = jnp.concatenate([w_out[:, n * wide : (n + 1) * wide] for n in range(width // wide)], axis=0)
    second = jnp.concatenate([w_gate, stacked], axis=1)

    first_own = gathered_y(first)
    first_other = swapped(first_own)
    normed = normed_tokens(tokens.reshape(seqs * local_len, width), pre_gain, where)
    qfv = project_heads(normed, first_own, first_other, seqs, local_len)
    qfv = qfv.reshape(seqs * HEADS, local_len, 3 * HK)
    second, qfv = lax.optimization_barrier((second, qfv))
    qfv = lax.all_to_all(qfv, SP, 0, 0, tiled=True)
    length = qfv.shape[0] * local_len
    qfv = qfv.reshape(length, 3 * HK)

    second_own = gathered_y(second)
    second_other = swapped(second_own)
    gate, weight = gate_and_weight(where, normed, second_own, second_other, width)

    head = lax.axis_index("x")
    gap = lax.dynamic_slice_in_dim((1.0 - lower_bound).reshape(HEADS, HK), head, 1, 0)
    run = jnp.cumsum(extra_decay.reshape(length // CHUNK, CHUNK), axis=1)
    state = initial_state[0].T
    heads = recurred(qfv, run, gap, state, norm_gain.reshape(1, HV))
    heads = lax.all_to_all(heads.reshape(seqs * HEADS, local_len, HV), SP, 0, 0, tiled=True)
    heads = heads.reshape(seqs, HEADS, local_len, HV)
    return output_rows(heads, gate, weight, post_gain)


def solution(mesh):
    split = Mesh(mesh.devices.reshape(8, 4, 8, 2), ("z", "x", "y", "c"))
    in_specs = (
        P(DP, SP, None),
        P(),
        P(DP, None),
        P(DP, None),
        P(DP, None),
        P(DP, None),
        P(),
        P(DP_SP, None),
        P(DP_SP, None, None),
        P(),
        P(DP, None),
        P(),
    )
    out_specs = P(DP, SP, None)
    return jax.shard_map(body, mesh=split, in_specs=in_specs, out_specs=out_specs, check_vma=False)
```

```python
import jax
import jax.numpy as jnp
from jax import lax
from jax.experimental import pallas as pl
from jax.experimental.pallas import tpu as pltpu
from jax.sharding import Mesh
from jax.sharding import PartitionSpec as P


HEADS = 4
HK = 128
HV = 128
CHUNK = 64
PAIR = 2 * CHUNK
TAIL = 8
SP = ("z", "x")
DP = ("y", "c")
DP_SP = ("y", "c", "z", "x")
OFFSETS = (0, -1, 1, -2, 2, -3, 3, 4)
ROWS = 128
OUT_ROWS = 32
EPS = 1e-06


F32 = jnp.float32
BF16 = jnp.bfloat16


def shifted(a, step):
    size = lax.axis_size("y")
    return lax.ppermute(a, "y", [(i, (i + step) % size) for i in range(size)])


def swapped(a):
    return lax.ppermute(a, "c", [(0, 1), (1, 0)])


def after(values, others):
    return lax.optimization_barrier((*values, *others))[: len(values)]


def gathered_y(shard, waits):
    pieces = [shard]
    up = down = shard
    for k in range(3):
        up, down = after((up, down), waits[k]) if waits[k] else (up, down)
        up, down = shifted(up, 1), shifted(down, -1)
        pieces += [up, down]
    up, down = after((up, down), waits[3]) if waits[3] else (up, down)
    half = shard.shape[0] // 2
    up, down = up[:half], down[half:]
    pieces += [shifted(up, 1), shifted(down, -1)]
    return stacked_pieces(pieces)


def stack_kernel(*refs):
    out_ref = refs[-1]
    first = 0
    for ref in refs[:-1]:
        rows = ref.shape[0]
        out_ref[first : first + rows, :] = ref[...]
        first += rows


def stacked_pieces(pieces):
    rows = sum(p.shape[0] for p in pieces)
    return pl.pallas_call(
        stack_kernel,
        in_specs=[vmem_spec()] * len(pieces),
        out_specs=vmem_spec(),
        out_shape=jax.ShapeDtypeStruct((rows, pieces[0].shape[1]), BF16),
        compiler_params=limit(8),
        name="stack",
    )(*pieces)


def dot(a, b):
    return jnp.dot(a, b, preferred_element_type=F32)


def dot_nt(a, b):
    return lax.dot_general(a, b, (((1,), (1,)), ((), ())), preferred_element_type=F32)


def dot_tn(a, b):
    return lax.dot_general(a, b, (((0,), (0,)), ((), ())), preferred_element_type=F32)


def sigmoid(a):
    return 0.5 * jnp.tanh(0.5 * a) + 0.5


def place(where_ref, j):
    core = where_ref[1] if j < len(OFFSETS) else 1 - where_ref[1]
    return 2 * ((where_ref[0] + OFFSETS[j % len(OFFSETS)] + 8) & 7) + core


def norm_kernel(where_ref, x_ref, gain_ref, out_ref):
    x = x_ref[...].astype(F32)
    scale = lax.rsqrt(jnp.mean(x * x, axis=-1, keepdims=True) + EPS)
    rows = pl.ds(pl.multiple_of(pl.program_id(0) * x.shape[0], x.shape[0]), x.shape[0])
    for j in range(2 * len(OFFSETS)):
        start = pl.multiple_of(place(where_ref, j) * ROWS, ROWS)
        part = x_ref[:, pl.ds(start, ROWS)].astype(F32) * scale * gain_ref[:, pl.ds(start, ROWS)]
        out_ref[rows, j * ROWS : (j + 1) * ROWS] = part.astype(BF16)


def normed_tokens(tokens, pre_gain, where):
    rows, width = tokens.shape
    tile = 128
    return pl.pallas_call(
        norm_kernel,
        grid_spec=pltpu.PrefetchScalarGridSpec(
            num_scalar_prefetch=1,
            grid=(rows // tile,),
            in_specs=[
                pl.BlockSpec((tile, width), lambda i, b: (i, 0)),
                pl.BlockSpec((1, width), lambda i, b: (0, 0)),
            ],
            out_specs=pl.BlockSpec(memory_space=pltpu.VMEM),
        ),
        out_shape=jax.ShapeDtypeStruct((rows, width), BF16),
        compiler_params=pltpu.CompilerParams(vmem_limit_bytes=6 << 20),
        name="norm",
    )(where, tokens, pre_gain.reshape(1, width))


def vmem_spec():
    return pl.BlockSpec(memory_space=pltpu.VMEM)


def limit(mib):
    return pltpu.CompilerParams(vmem_limit_bytes=mib << 20)


def project_kernel(a_ref, own_ref, other_ref, out_ref):
    half = own_ref.shape[0]
    seqs, heads, _, local_len, _ = out_ref.shape
    wide = heads * HK
    cols = pl.ds(pl.multiple_of(pl.program_id(0) * wide, wide), wide)
    total = dot(a_ref[:, :half], own_ref[:, cols]) + dot(a_ref[:, half:], other_ref[:, cols])
    total = total.astype(BF16)
    for n in range(heads):
        out_ref[:, n, 0] = total[:, n * HK : (n + 1) * HK].reshape(seqs, local_len, HK)


def project_heads(normed, own, other, seqs, local_len):
    block = (seqs, 2, 1, local_len, HK)
    return pl.pallas_call(
        project_kernel,
        grid=(HEADS,),
        in_specs=[vmem_spec()] * 3,
        out_specs=pl.BlockSpec(block, lambda j: (0, j % 2, j // 2, 0, 0)),
        out_shape=pltpu.HBM((seqs, HEADS, 2, local_len, HK), BF16),
        compiler_params=limit(8),
        name="project",
    )(normed, own, other)


def pair_masks():
    row = lax.broadcasted_iota(jnp.int32, (PAIR, PAIR), 0)
    col = lax.broadcasted_iota(jnp.int32, (PAIR, PAIR), 1)
    causal = (row >= col) & ((row < CHUNK) == (col < CHUNK))
    return causal, row < CHUNK, col < CHUNK


def keys_and_total(f, gap, ones):
    keys = gap * sigmoid(-f)
    decay = jnp.log1p(-keys)
    high = decay.astype(BF16)
    low = (decay - high.astype(F32)).astype(BF16)
    return keys, dot(ones, high) + dot(ones, low)


def state_kernel(fv_ref, run_ref, tail_ref, gap_ref, state_ref, out_ref, carry_ref):
    chunks = out_ref.shape[0]
    causal, first_row, _ = pair_masks()
    ones = causal.astype(F32).astype(BF16)
    gap = gap_ref[...]
    block = pl.program_id(0)

    @pl.when(block == 0)
    def _():
        carry_ref[...] = state_ref[...]

    state = carry_ref[...]
    for p in range(chunks // 2):
        b = block * chunks + 2 * p
        f = fv_ref[pl.ds(b, 2), 0].reshape(PAIR, HK).astype(F32)
        keys, total = keys_and_total(f, gap, ones)
        run_row = run_ref[pl.ds(block * (chunks // 2) + p, 1), :]
        run = jnp.broadcast_to(run_row, (PAIR, PAIR)).T
        ends = [total[n * CHUNK + CHUNK - 1 : (n + 1) * CHUNK, :] for n in range(2)]
        run_ends = [run[n * CHUNK + CHUNK - 1 : (n + 1) * CHUNK, :] for n in range(2)]
        end = jnp.where(first_row, ends[0], ends[1])
        run_end = jnp.where(first_row, run_ends[0], run_ends[1])
        weighted = (keys * jnp.exp((end - total) + (run_end - run))).astype(BF16)
        for n in range(2):
            out_ref[2 * p + n, 0:HV, :] = state.astype(BF16)
            out_ref[2 * p + n, HV:, :] = tail_ref[b + n]
            rows = slice(n * CHUNK, (n + 1) * CHUNK)
            added = dot_tn(fv_ref[b + n, 1], weighted[rows])
            state = state * jnp.exp(ends[n] + run_ends[n]) + added
    carry_ref[...] = state


def chunk_states(fv, run, tail, gap, state):
    chunks = fv.shape[0]
    group = 8
    return pl.pallas_call(
        state_kernel,
        grid=(chunks // group,),
        in_specs=[
            vmem_spec(),
            pl.BlockSpec(run.shape, lambda i: (0, 0)),
            pl.BlockSpec(tail.shape, lambda i: (0, 0, 0)),
            pl.BlockSpec(gap.shape, lambda i: (0, 0)),
            pl.BlockSpec(state.shape, lambda i: (0, 0)),
        ],
        out_specs=pl.BlockSpec((group, HV + TAIL, HK), lambda i: (i, 0, 0)),
        out_shape=pltpu.HBM((chunks, HV + TAIL, HK), BF16),
        scratch_shapes=[pltpu.VMEM((HV, HK), F32)],
        compiler_params=limit(6),
        name="state",
    )(fv, run, tail, gap, state)


def local_kernel(a_ref, own_ref, other_ref, fv_ref, gap_ref, out_ref):
    half = own_ref.shape[0]
    seqs, heads, _, _, _ = fv_ref.shape
    wide = heads * HK
    causal, _, _ = pair_masks()
    ones = causal.astype(F32).astype(BF16)
    total_q = dot(a_ref[:, :half], own_ref[:, :wide]) + dot(a_ref[:, half:], other_ref[:, :wide])
    q_pre = total_q.astype(BF16)
    total_g = dot(a_ref[:, :half], own_ref[:, wide : 2 * wide])
    total_g += dot(a_ref[:, half:], other_ref[:, wide : 2 * wide])
    g_pre = total_g.astype(BF16)
    for p in range(seqs // 2):
        for h in range(heads):
            q = q_pre[p * PAIR : (p + 1) * PAIR, h * HK : (h + 1) * HK].astype(F32)
            f = fv_ref[2 * p : 2 * p + 2, h, 0].reshape(PAIR, HK).astype(F32)
            keys, total = keys_and_total(f, gap_ref[h : h + 1, :], ones)
            q_scaled = (q * sigmoid(q) * jnp.exp(total)).astype(BF16)
            k_scaled = (keys * jnp.exp(-total)).astype(BF16)
            out_ref[0, p, h] = q_scaled
            out_ref[1, p, h] = jnp.where(causal, dot_nt(q_scaled, k_scaled), 0.0).astype(BF16)
            out_ref[2, p, h] = g_pre[p * PAIR : (p + 1) * PAIR, h * HV : (h + 1) * HV]


def weight_kernel(where_ref, own_ref, other_ref, weight_ref):
    wide = HEADS * HV
    for k, stack in enumerate((own_ref, other_ref)):
        for j in range(len(OFFSETS)):
            start = pl.multiple_of(place(where_ref, k * len(OFFSETS) + j) * OUT_ROWS, OUT_ROWS)
            for n in range(ROWS // OUT_ROWS):
                first = j * ROWS + n * OUT_ROWS
                weight_ref[pl.ds(start, OUT_ROWS), n * wide : (n + 1) * wide] = stack[
                    first : first + OUT_ROWS, 2 * wide :
                ]


def local_parts(normed, own, other, fv, gap):
    seqs, heads, _, _, _ = fv.shape
    return pl.pallas_call(
        local_kernel,
        in_specs=[vmem_spec()] * 5,
        out_shape=pltpu.HBM((3, seqs // 2, heads, PAIR, HK), BF16),
        compiler_params=limit(14),
        name="local",
    )(normed, own, other, fv, gap)


def out_weight(where, own, other, width):
    return pl.pallas_call(
        weight_kernel,
        in_specs=[pl.BlockSpec(memory_space=pltpu.SMEM)] + [vmem_spec()] * 2,
        out_specs=vmem_spec(),
        out_shape=jax.ShapeDtypeStruct((HEADS * HV, width), BF16),
        compiler_params=limit(4),
        name="weight",
    )(where, own, other)


def output_kernel(state_ref, part_ref, fv_ref, weight_ref, norm_ref, post_ref, out_ref):
    heads = fv_ref.shape[1]
    pairs = out_ref.shape[0] // 2
    _, _, first_col = pair_masks()
    gain = norm_ref[...]
    rows = []
    for n_pair in range(pairs):
        p = n_pair
        gated = []
        for h in range(heads):
            runs, carried = [], []
            for n in range(2):
                s = pl.program_id(0) * 2 * pairs + 2 * p + n
                tail = state_ref[s, h, HV:, :].astype(F32)
                runs.append(tail[0:1, :] + tail[1:2, :] + tail[2:3, :])
                query = part_ref[0, p, h, n * CHUNK : (n + 1) * CHUNK, :]
                carried.append(dot_nt(query, state_ref[s, h, 0:HV, :]))
            run = jnp.where(first_col, runs[0], runs[1])
            run_cols = run.T
            weight = jnp.exp(jnp.minimum(run_cols - run, 0.0))
            scores = (part_ref[1, p, h].astype(F32) * weight).astype(BF16)
            v = fv_ref[2 * p : 2 * p + 2, h, 0].reshape(PAIR, HV)
            out = jnp.concatenate(carried, axis=0) * jnp.exp(run_cols) + dot(scores, v)
            scale = lax.rsqrt(jnp.mean(out * out, axis=-1, keepdims=True) + EPS)
            head = (out * scale * gain).astype(BF16).astype(F32)
            gate = part_ref[2, p, h].astype(F32)
            gated.append((head * (gate * sigmoid(gate))).astype(BF16))
        rows.append(jnp.concatenate(gated, axis=1))
    mixed = dot(jnp.concatenate(rows, axis=0), weight_ref[...])
    scale = lax.rsqrt(jnp.mean(mixed * mixed, axis=-1, keepdims=True) + EPS)
    out_ref[...] = (mixed * scale * post_ref[...]).astype(BF16).reshape(out_ref.shape)


def output_rows(states, parts, fv, weight, norm_gain, post_gain):
    seqs, heads, _, local_len, _ = fv.shape
    width = weight.shape[1]
    group = 4
    return pl.pallas_call(
        output_kernel,
        grid=(seqs // group,),
        in_specs=[
            vmem_spec(),
            pl.BlockSpec((3, group // 2, heads, PAIR, HK), lambda i: (0, i, 0, 0, 0)),
            pl.BlockSpec((group, heads, 1, local_len, HK), lambda i: (i, 0, 1, 0, 0)),
            vmem_spec(),
            vmem_spec(),
            vmem_spec(),
        ],
        out_specs=pl.BlockSpec((group, local_len, width), lambda i: (i, 0, 0)),
        out_shape=jax.ShapeDtypeStruct((seqs, local_len, width), BF16),
        compiler_params=limit(12),
        name="output",
    )(states, parts, fv, weight, norm_gain.reshape(1, HV), post_gain.reshape(1, width))


def layer(
    tokens,
    pre_gain,
    w_query,
    w_forget,
    w_value,
    w_gate,
    lower_bound,
    extra_decay,
    initial_state,
    norm_gain,
    w_out,
    post_gain,
):
    seqs, local_len, width = tokens.shape
    items = seqs * HEADS
    wide = HEADS * HV
    where = jnp.stack([lax.axis_index("y"), lax.axis_index("c")]).astype(jnp.int32)
    gaps = (1.0 - lower_bound).reshape(HEADS, HK)

    first = jnp.concatenate([w_forget, w_value], axis=1)
    stacked = [w_out[:, n * wide : (n + 1) * wide] for n in range(width // wide)]
    second = jnp.concatenate([w_query, w_gate, jnp.concatenate(stacked, axis=0)], axis=1)
    gap = lax.dynamic_slice_in_dim(gaps, lax.axis_index("x"), 1, 0)
    run = jnp.cumsum(extra_decay.reshape(items, CHUNK), axis=1)
    high = lax.reduce_precision(run, 8, 7)
    middle = lax.reduce_precision(run - high, 8, 7)
    low = run - high - middle
    tail = jnp.stack([high, middle, low] + [jnp.zeros_like(high)] * (TAIL - 3), axis=1)
    tail = jnp.concatenate([tail, tail], axis=2).astype(BF16)
    run = run.reshape(items // 2, PAIR)
    state = initial_state[0].T
    normed = normed_tokens(tokens.reshape(seqs * local_len, width), pre_gain, where)

    early = (second, gap, run, tail, state, normed)
    first_own = gathered_y(first, ((), (), early, ()))
    first_other = swapped(first_own)
    fv = project_heads(normed, first_own, first_other, seqs, local_len)
    moved = lax.all_to_all(fv.reshape(items, 2 * local_len, HK), SP, 0, 0, tiled=True)
    starts = chunk_states(moved.reshape(items, 2, local_len, HK), run, tail, gap, state)
    states = lax.all_to_all(starts, SP, 0, 0, tiled=True)

    second_own = gathered_y(second, ((first_own,), (fv,), (), (starts,)))
    second_other = swapped(second_own)
    parts = local_parts(normed, second_own, second_other, fv, gaps)
    weight = out_weight(where, second_own, second_other, width)
    states = states.reshape(seqs, HEADS, HV + TAIL, HK)
    return output_rows(states, parts, fv, weight, norm_gain, post_gain)


def solution(mesh):
    split = Mesh(mesh.devices.reshape(8, 4, 8, 2), ("z", "x", "y", "c"))
    in_specs = (
        P(DP, SP, None),
        P(),
        P(DP, None),
        P(DP, None),
        P(DP, None),
        P(DP, None),
        P(),
        P(DP_SP, None),
        P(DP_SP, None, None),
        P(),
        P(DP, None),
        P(),
    )
    out_specs = P(DP, SP, None)
    return jax.shard_map(layer, mesh=split, in_specs=in_specs, out_specs=out_specs, check_vma=False)
```

```python
import functools

import jax
import jax.numpy as jnp
from jax import lax
from jax.experimental import pallas as pl
from jax.experimental.pallas import tpu as pltpu
from jax.sharding import Mesh
from jax.sharding import PartitionSpec as P


HEADS = 4
HK = 128
HV = 128
CHUNK = 64
PAIR = 2 * CHUNK
TAIL = 8
SP = ("z", "x")
DP = ("y", "c")
DP_SP = ("y", "c", "z", "x")
OFFSETS = (0, -1, 1, -2, 2, -3, 3, 4)
ROWS = 128
OUT_ROWS = 32
EPS = 1e-06
WIDE = HEADS * HV


F32 = jnp.float32
BF16 = jnp.bfloat16


def shifted(a, step):
    size = lax.axis_size("y")
    return lax.ppermute(a, "y", [(i, (i + step) % size) for i in range(size)])


def swapped(a):
    return lax.ppermute(a, "c", [(0, 1), (1, 0)])


def after(values, others):
    return lax.optimization_barrier((*values, *others))[: len(values)]


def gathered_y(shard, waits):
    pieces = [shard]
    own, other = [], []
    up = down = shard
    for k in range(4):
        up, down = after((up, down), waits[k]) if waits[k] else (up, down)
        up = shifted(up, 1)
        down = shifted(down, -1) if k < 3 else None
        if k in (2, 3):
            own.append(stacked_pieces(pieces) if len(pieces) > 1 else pieces[0])
            other.append(swapped(own[-1]))
            pieces = []
        pieces += [up, down] if k < 3 else [up]
    own.append(pieces[0])
    other.append(swapped(pieces[0]))
    return own, other


def in_hbm(a):
    return pltpu.with_memory_space_constraint(a, pltpu.HBM)


def join_kernel(*refs, places):
    out_ref, sems = refs[-2:]
    copies = []
    for n, (k, (rows, cols), (r, c)) in enumerate(places):
        source = refs[k].at[:, pl.ds(cols, WIDE)]
        target = out_ref.at[pl.ds(r, source.shape[0]), pl.ds(c, WIDE)]
        copies.append(pltpu.make_async_copy(source, target, sems.at[n]))
    for copy in copies:
        copy.start()
    for copy in copies:
        copy.wait()


def joined(arrays, places, width):
    return pl.pallas_call(
        functools.partial(join_kernel, places=places),
        in_specs=[pl.BlockSpec(memory_space=pl.ANY)] * len(arrays),
        out_specs=vmem_spec(),
        out_shape=jax.ShapeDtypeStruct((ROWS, width), BF16),
        scratch_shapes=[pltpu.SemaphoreType.DMA((len(places),))],
        compiler_params=limit(2),
    )(*[in_hbm(a) for a in arrays])


def stack_kernel(*refs):
    out_ref = refs[-1]
    first = 0
    for ref in refs[:-1]:
        rows = ref.shape[0]
        out_ref[first : first + rows, :] = ref[...]
        first += rows


def stacked_pieces(pieces):
    rows = sum(p.shape[0] for p in pieces)
    return pl.pallas_call(
        stack_kernel,
        in_specs=[vmem_spec()] * len(pieces),
        out_specs=vmem_spec(),
        out_shape=jax.ShapeDtypeStruct((rows, pieces[0].shape[1]), BF16),
        compiler_params=limit(6),
        name="stack",
    )(*pieces)


def against(a_ref, refs, cols):
    total = None
    first = 0
    for ref in refs:
        rows = ref.shape[0]
        part = dot(a_ref[:, first : first + rows], ref[:, cols])
        total = part if total is None else total + part
        first += rows
    return total


def dot(a, b):
    return jnp.dot(a, b, preferred_element_type=F32)


def dot_nt(a, b):
    return lax.dot_general(a, b, (((1,), (1,)), ((), ())), preferred_element_type=F32)


def dot_tn(a, b):
    return lax.dot_general(a, b, (((0,), (0,)), ((), ())), preferred_element_type=F32)


def sigmoid(a):
    return 0.5 * jnp.tanh(0.5 * a) + 0.5


def place(where_ref, j):
    core = where_ref[1] if j < len(OFFSETS) else 1 - where_ref[1]
    return 2 * ((where_ref[0] + OFFSETS[j % len(OFFSETS)] + 8) & 7) + core


def norm_kernel(where_ref, x_ref, gain_ref, out_ref):
    x = x_ref[...].astype(F32)
    scale = lax.rsqrt(jnp.mean(x * x, axis=-1, keepdims=True) + EPS)
    rows = pl.ds(pl.multiple_of(pl.program_id(0) * x.shape[0], x.shape[0]), x.shape[0])
    for j in range(2 * len(OFFSETS)):
        start = pl.multiple_of(place(where_ref, j) * ROWS, ROWS)
        part = x_ref[:, pl.ds(start, ROWS)].astype(F32) * scale * gain_ref[:, pl.ds(start, ROWS)]
        out_ref[rows, j * ROWS : (j + 1) * ROWS] = part.astype(BF16)


def normed_tokens(tokens, pre_gain, where):
    rows, width = tokens.shape
    tile = 128
    return pl.pallas_call(
        norm_kernel,
        grid_spec=pltpu.PrefetchScalarGridSpec(
            num_scalar_prefetch=1,
            grid=(rows // tile,),
            in_specs=[
                pl.BlockSpec((tile, width), lambda i, b: (i, 0)),
                pl.BlockSpec((1, width), lambda i, b: (0, 0)),
            ],
            out_specs=pl.BlockSpec(memory_space=pltpu.VMEM),
        ),
        out_shape=jax.ShapeDtypeStruct((rows, width), BF16),
        compiler_params=pltpu.CompilerParams(vmem_limit_bytes=6 << 20),
        name="norm",
    )(where, in_hbm(tokens), pre_gain.reshape(1, width))


def vmem_spec():
    return pl.BlockSpec(memory_space=pltpu.VMEM)


def limit(mib):
    return pltpu.CompilerParams(vmem_limit_bytes=mib << 20)


def project_kernel(a_ref, *refs):
    out_ref = refs[-1]
    seqs, heads, _, local_len, _ = out_ref.shape
    wide = heads * HK
    cols = pl.ds(pl.multiple_of(pl.program_id(0) * wide, wide), wide)
    total = against(a_ref, refs[:-1], cols).astype(BF16)
    for n in range(heads):
        out_ref[:, n, 0] = total[:, n * HK : (n + 1) * HK].reshape(seqs, local_len, HK)


def project_heads(normed, stacks, seqs, local_len):
    block = (seqs, 2, 1, local_len, HK)
    return pl.pallas_call(
        project_kernel,
        grid=(HEADS,),
        in_specs=[vmem_spec()] * (1 + len(stacks)),
        out_specs=pl.BlockSpec(block, lambda j: (0, j % 2, j // 2, 0, 0)),
        out_shape=pltpu.HBM((seqs, HEADS, 2, local_len, HK), BF16),
        compiler_params=limit(8),
        name="project",
    )(normed, *stacks)


def pair_masks():
    row = lax.broadcasted_iota(jnp.int32, (PAIR, PAIR), 0)
    col = lax.broadcasted_iota(jnp.int32, (PAIR, PAIR), 1)
    causal = (row >= col) & ((row < CHUNK) == (col < CHUNK))
    return causal, row < CHUNK, col < CHUNK


def keys_and_total(f, gap, ones):
    keys = gap * sigmoid(-f)
    decay = jnp.log1p(-keys)
    high = decay.astype(BF16)
    low = (decay - high.astype(F32)).astype(BF16)
    return keys, dot(ones, high) + dot(ones, low)


def state_kernel(fv_ref, run_ref, tail_ref, gap_ref, state_ref, out_ref, carry_ref):
    chunks = out_ref.shape[0]
    causal, first_row, _ = pair_masks()
    ones = causal.astype(F32).astype(BF16)
    gap = gap_ref[...]
    block = pl.program_id(0)

    @pl.when(block == 0)
    def _():
        carry_ref[...] = state_ref[...]

    state = carry_ref[...]
    for p in range(chunks // 2):
        b = block * chunks + 2 * p
        f = fv_ref[pl.ds(b, 2), 0].reshape(PAIR, HK).astype(F32)
        keys, total = keys_and_total(f, gap, ones)
        run_row = run_ref[pl.ds(block * (chunks // 2) + p, 1), :]
        run = jnp.broadcast_to(run_row, (PAIR, PAIR)).T
        ends = [total[n * CHUNK + CHUNK - 1 : (n + 1) * CHUNK, :] for n in range(2)]
        run_ends = [run[n * CHUNK + CHUNK - 1 : (n + 1) * CHUNK, :] for n in range(2)]
        end = jnp.where(first_row, ends[0], ends[1])
        run_end = jnp.where(first_row, run_ends[0], run_ends[1])
        weighted = (keys * jnp.exp((end - total) + (run_end - run))).astype(BF16)
        for n in range(2):
            out_ref[2 * p + n, 0:HV, :] = state.astype(BF16)
            out_ref[2 * p + n, HV:, :] = tail_ref[b + n]
            rows = slice(n * CHUNK, (n + 1) * CHUNK)
            added = dot_tn(fv_ref[b + n, 1], weighted[rows])
            state = state * jnp.exp(ends[n] + run_ends[n]) + added
    carry_ref[...] = state


def chunk_states(fv, run, tail, gap, state):
    chunks = fv.shape[0]
    group = 8
    return pl.pallas_call(
        state_kernel,
        grid=(chunks // group,),
        in_specs=[
            vmem_spec(),
            pl.BlockSpec(run.shape, lambda i: (0, 0)),
            pl.BlockSpec(tail.shape, lambda i: (0, 0, 0)),
            pl.BlockSpec(gap.shape, lambda i: (0, 0)),
            pl.BlockSpec(state.shape, lambda i: (0, 0)),
        ],
        out_specs=pl.BlockSpec((group, HV + TAIL, HK), lambda i: (i, 0, 0)),
        out_shape=pltpu.HBM((chunks, HV + TAIL, HK), BF16),
        scratch_shapes=[pltpu.VMEM((HV, HK), F32)],
        compiler_params=limit(6),
        name="state",
    )(fv, in_hbm(run), in_hbm(tail), in_hbm(gap), in_hbm(state))


def local_kernel(a_ref, fv_ref, gap_ref, *refs):
    out_ref, stacks = refs[-1], refs[:-1]
    seqs, heads, _, _, _ = fv_ref.shape
    wide = heads * HK
    causal, _, _ = pair_masks()
    ones = causal.astype(F32).astype(BF16)
    q_pre = against(a_ref, stacks, slice(0, wide)).astype(BF16)
    g_pre = against(a_ref, stacks, slice(wide, 2 * wide)).astype(BF16)
    for p in range(seqs // 2):
        for h in range(heads):
            q = q_pre[p * PAIR : (p + 1) * PAIR, h * HK : (h + 1) * HK].astype(F32)
            f = fv_ref[2 * p : 2 * p + 2, h, 0].reshape(PAIR, HK).astype(F32)
            keys, total = keys_and_total(f, gap_ref[h : h + 1, :], ones)
            q_scaled = (q * sigmoid(q) * jnp.exp(total)).astype(BF16)
            k_scaled = (keys * jnp.exp(-total)).astype(BF16)
            out_ref[0, p, h] = q_scaled
            out_ref[1, p, h] = jnp.where(causal, dot_nt(q_scaled, k_scaled), 0.0).astype(BF16)
            out_ref[2, p, h] = g_pre[p * PAIR : (p + 1) * PAIR, h * HV : (h + 1) * HV]


def weight_kernel(where_ref, *refs):
    weight_ref = refs[-1]
    j = 0
    for stack in refs[:-1]:
        for first in range(0, stack.shape[0], ROWS):
            start = pl.multiple_of(place(where_ref, j) * OUT_ROWS, OUT_ROWS)
            for n in range(ROWS // OUT_ROWS):
                rows = slice(first + n * OUT_ROWS, first + (n + 1) * OUT_ROWS)
                weight_ref[pl.ds(start, OUT_ROWS), n * WIDE : (n + 1) * WIDE] = stack[rows, 2 * WIDE :]
            j += 1


def local_parts(normed, stacks, fv, gap):
    seqs, heads, _, _, _ = fv.shape
    return pl.pallas_call(
        local_kernel,
        in_specs=[vmem_spec()] * (3 + len(stacks)),
        out_shape=pltpu.HBM((3, seqs // 2, heads, PAIR, HK), BF16),
        compiler_params=limit(14),
        name="local",
    )(normed, fv, gap, *stacks)


def out_weight(where, stacks, width):
    return pl.pallas_call(
        weight_kernel,
        in_specs=[pl.BlockSpec(memory_space=pltpu.SMEM)] + [vmem_spec()] * len(stacks),
        out_specs=vmem_spec(),
        out_shape=jax.ShapeDtypeStruct((WIDE, width), BF16),
        compiler_params=limit(4),
        name="weight",
    )(where, *stacks)


def output_kernel(state_ref, part_ref, fv_ref, weight_ref, norm_ref, post_ref, out_ref):
    heads = fv_ref.shape[1]
    pairs = out_ref.shape[0] // 2
    _, _, first_col = pair_masks()
    gain = norm_ref[...]
    rows = []
    for n_pair in range(pairs):
        p = n_pair
        gated = []
        for h in range(heads):
            runs, carried = [], []
            for n in range(2):
                s = pl.program_id(0) * 2 * pairs + 2 * p + n
                tail = state_ref[s, h, HV:, :].astype(F32)
                runs.append(tail[0:1, :] + tail[1:2, :] + tail[2:3, :])
                query = part_ref[0, p, h, n * CHUNK : (n + 1) * CHUNK, :]
                carried.append(dot_nt(query, state_ref[s, h, 0:HV, :]))
            run = jnp.where(first_col, runs[0], runs[1])
            run_cols = run.T
            weight = jnp.exp(jnp.minimum(run_cols - run, 0.0))
            scores = (part_ref[1, p, h].astype(F32) * weight).astype(BF16)
            v = fv_ref[2 * p : 2 * p + 2, h, 0].reshape(PAIR, HV)
            out = jnp.concatenate(carried, axis=0) * jnp.exp(run_cols) + dot(scores, v)
            scale = lax.rsqrt(jnp.mean(out * out, axis=-1, keepdims=True) + EPS)
            head = (out * scale * gain).astype(BF16).astype(F32)
            gate = part_ref[2, p, h].astype(F32)
            gated.append((head * (gate * sigmoid(gate))).astype(BF16))
        rows.append(jnp.concatenate(gated, axis=1))
    mixed = dot(jnp.concatenate(rows, axis=0), weight_ref[...])
    scale = lax.rsqrt(jnp.mean(mixed * mixed, axis=-1, keepdims=True) + EPS)
    out_ref[...] = (mixed * scale * post_ref[...]).astype(BF16).reshape(out_ref.shape)


def output_rows(states, parts, fv, weight, norm_gain, post_gain):
    seqs, heads, _, local_len, _ = fv.shape
    width = weight.shape[1]
    group = 4
    return pl.pallas_call(
        output_kernel,
        grid=(seqs // group,),
        in_specs=[
            vmem_spec(),
            pl.BlockSpec((3, group // 2, heads, PAIR, HK), lambda i: (0, i, 0, 0, 0)),
            pl.BlockSpec((group, heads, 1, local_len, HK), lambda i: (i, 0, 1, 0, 0)),
            vmem_spec(),
            vmem_spec(),
            vmem_spec(),
        ],
        out_specs=pl.BlockSpec((group, local_len, width), lambda i: (i, 0, 0)),
        out_shape=jax.ShapeDtypeStruct((seqs, local_len, width), BF16),
        compiler_params=limit(12),
        name="output",
    )(states, in_hbm(parts), in_hbm(fv), weight, norm_gain.reshape(1, HV), post_gain.reshape(1, width))


def layer(
    tokens,
    pre_gain,
    w_query,
    w_forget,
    w_value,
    w_gate,
    lower_bound,
    extra_decay,
    initial_state,
    norm_gain,
    w_out,
    post_gain,
):
    seqs, local_len, width = tokens.shape
    items = seqs * HEADS
    where = jnp.stack([lax.axis_index("y"), lax.axis_index("c")]).astype(jnp.int32)
    gaps = (1.0 - lower_bound).reshape(HEADS, HK)

    first = joined((w_forget, w_value), ((0, (0, 0), (0, 0)), (1, (0, 0), (0, WIDE))), 2 * WIDE)
    places = [(0, (0, 0), (0, 0)), (1, (0, 0), (0, WIDE))]
    places += [(2, (0, n * WIDE), (n * OUT_ROWS, 2 * WIDE)) for n in range(width // WIDE)]
    second = joined((w_query, w_gate, w_out), tuple(places), 3 * WIDE)
    gap = lax.dynamic_slice_in_dim(gaps, lax.axis_index("x"), 1, 0)
    run = jnp.cumsum(extra_decay.reshape(items, CHUNK), axis=1)
    high = lax.reduce_precision(run, 8, 7)
    middle = lax.reduce_precision(run - high, 8, 7)
    low = run - high - middle
    tail = jnp.stack([high, middle, low] + [jnp.zeros_like(high)] * (TAIL - 3), axis=1)
    tail = jnp.concatenate([tail, tail], axis=2).astype(BF16)
    run = run.reshape(items // 2, PAIR)
    state = initial_state[0].T
    normed = normed_tokens(tokens.reshape(seqs * local_len, width), pre_gain, where)

    first_own, first_other = gathered_y(first, ((), (normed,), (second,), ()))
    fv = project_heads(normed, first_own + first_other, seqs, local_len)
    moved = lax.all_to_all(fv.reshape(items, 2 * local_len, HK), SP, 0, 0, tiled=True)
    starts = chunk_states(moved.reshape(items, 2, local_len, HK), run, tail, gap, state)
    states = lax.all_to_all(starts, SP, 0, 0, tiled=True)

    second_own, second_other = gathered_y(second, ((), (), (), ()))
    stacks = second_own + second_other
    parts = local_parts(normed, stacks, fv, gaps)
    weight = out_weight(where, stacks, width)
    states = states.reshape(seqs, HEADS, HV + TAIL, HK)
    return output_rows(states, parts, fv, weight, norm_gain, post_gain)


def solution(mesh):
    split = Mesh(mesh.devices.reshape(8, 4, 8, 2), ("z", "x", "y", "c"))
    in_specs = (
        P(DP, SP, None),
        P(),
        P(DP, None),
        P(DP, None),
        P(DP, None),
        P(DP, None),
        P(),
        P(DP_SP, None),
        P(DP_SP, None, None),
        P(),
        P(DP, None),
        P(),
    )
    out_specs = P(DP, SP, None)
    return jax.shard_map(layer, mesh=split, in_specs=in_specs, out_specs=out_specs, check_vma=False)
```

```python
import functools

import jax
import jax.numpy as jnp
from jax import lax
from jax.experimental import pallas as pl
from jax.experimental.pallas import tpu as pltpu
from jax.sharding import Mesh
from jax.sharding import PartitionSpec as P


HEADS = 4
HK = 128
HV = 128
CHUNK = 64
PAIR = 2 * CHUNK
TAIL = 8
SP = ("z", "x")
DP = ("y", "c")
DP_SP = ("y", "c", "z", "x")
OFFSETS = (0, -1, 1, -2, 2, -3, 3, 4)
ROWS = 128
OUT_ROWS = 32
EPS = 1e-06
WIDE = HEADS * HV


F32 = jnp.float32
BF16 = jnp.bfloat16


def shifted(a, step):
    size = lax.axis_size("y")
    return lax.ppermute(a, "y", [(i, (i + step) % size) for i in range(size)])


def swapped(a):
    return lax.ppermute(a, "c", [(0, 1), (1, 0)])


def after(values, others):
    return lax.optimization_barrier((*values, *others))[: len(values)]


def gathered_y(shard, waits, halves):
    pieces = [shard]
    own, other = [], []
    up = down = shard
    for k in range(4):
        up, down = after((up, down), waits[k]) if waits[k] else (up, down)
        if k == 3 and halves:
            middle = shard.shape[0] // 2
            up, down = up[:middle], down[middle:]
        up = shifted(up, 1)
        if k < 3 or halves:
            down = shifted(down, -1)
        if k in (2, 3):
            own.append(stacked_pieces(pieces) if len(pieces) > 1 else pieces[0])
            other.append(swapped(own[-1]))
            pieces = []
        pieces += [up, down] if k < 3 or halves else [up]
    own.append(stacked_pieces(pieces) if halves else pieces[0])
    other.append(swapped(own[-1]))
    return own, other


def in_hbm(a):
    return pltpu.with_memory_space_constraint(a, pltpu.HBM)


def join_kernel(*refs, places):
    out_ref, sems = refs[-2:]
    copies = []
    for n, (k, (rows, cols), (r, c)) in enumerate(places):
        source = refs[k].at[:, pl.ds(cols, WIDE)]
        target = out_ref.at[pl.ds(r, source.shape[0]), pl.ds(c, WIDE)]
        copies.append(pltpu.make_async_copy(source, target, sems.at[n]))
    for copy in copies:
        copy.start()
    for copy in copies:
        copy.wait()


def joined(arrays, places, width):
    return pl.pallas_call(
        functools.partial(join_kernel, places=places),
        in_specs=[pl.BlockSpec(memory_space=pl.ANY)] * len(arrays),
        out_specs=vmem_spec(),
        out_shape=jax.ShapeDtypeStruct((ROWS, width), BF16),
        scratch_shapes=[pltpu.SemaphoreType.DMA((len(places),))],
        compiler_params=limit(2),
    )(*[in_hbm(a) for a in arrays])


def stack_kernel(*refs):
    out_ref = refs[-1]
    first = 0
    for ref in refs[:-1]:
        rows = ref.shape[0]
        out_ref[first : first + rows, :] = ref[...]
        first += rows


def stacked_pieces(pieces):
    rows = sum(p.shape[0] for p in pieces)
    return pl.pallas_call(
        stack_kernel,
        in_specs=[vmem_spec()] * len(pieces),
        out_specs=vmem_spec(),
        out_shape=jax.ShapeDtypeStruct((rows, pieces[0].shape[1]), BF16),
        compiler_params=limit(6),
        name="stack",
    )(*pieces)


def against(a_refs, refs, cols):
    return jnp.concatenate([rows_against(a_ref, refs, cols) for a_ref in a_refs], axis=0)


def rows_against(a_ref, refs, cols):
    total = None
    first = 0
    for ref in refs:
        rows = ref.shape[0]
        part = dot(a_ref[:, first : first + rows], ref[:, cols])
        total = part if total is None else total + part
        first += rows
    return total


def dot(a, b):
    return jnp.dot(a, b, preferred_element_type=F32)


def dot_nt(a, b):
    return lax.dot_general(a, b, (((1,), (1,)), ((), ())), preferred_element_type=F32)


def dot_tn(a, b):
    return lax.dot_general(a, b, (((0,), (0,)), ((), ())), preferred_element_type=F32)


def sigmoid(a):
    return 0.5 * jnp.tanh(0.5 * a) + 0.5


def place(where_ref, j):
    core = where_ref[1] if j < len(OFFSETS) else 1 - where_ref[1]
    return 2 * ((where_ref[0] + OFFSETS[j % len(OFFSETS)] + 8) & 7) + core


def norm_kernel(where_ref, x_ref, gain_ref, out_ref):
    x = x_ref[...].astype(F32)
    scale = lax.rsqrt(jnp.mean(x * x, axis=-1, keepdims=True) + EPS)
    rows = pl.ds(pl.multiple_of(pl.program_id(0) * x.shape[0], x.shape[0]), x.shape[0])
    for j in range(2 * len(OFFSETS)):
        start = pl.multiple_of(place(where_ref, j) * ROWS, ROWS)
        part = x_ref[:, pl.ds(start, ROWS)].astype(F32) * scale * gain_ref[:, pl.ds(start, ROWS)]
        out_ref[rows, j * ROWS : (j + 1) * ROWS] = part.astype(BF16)


def normed_tokens(tokens, pre_gain, where, half):
    rows, width = tokens.shape
    rows = rows // 2
    tile = 64
    skip = half * (rows // tile)
    return pl.pallas_call(
        norm_kernel,
        grid_spec=pltpu.PrefetchScalarGridSpec(
            num_scalar_prefetch=1,
            grid=(rows // tile,),
            in_specs=[
                pl.BlockSpec((tile, width), lambda i, b: (i + skip, 0)),
                pl.BlockSpec((1, width), lambda i, b: (0, 0)),
            ],
            out_specs=pl.BlockSpec(memory_space=pltpu.VMEM),
        ),
        out_shape=jax.ShapeDtypeStruct((rows, width), BF16),
        compiler_params=pltpu.CompilerParams(vmem_limit_bytes=6 << 20),
        name="norm",
    )(where, in_hbm(tokens), in_hbm(pre_gain.reshape(1, width)))


def vmem_spec():
    return pl.BlockSpec(memory_space=pltpu.VMEM)


def limit(mib):
    return pltpu.CompilerParams(vmem_limit_bytes=mib << 20)


def project_kernel(*refs):
    out_ref = refs[-1]
    seqs, heads, _, local_len, _ = out_ref.shape
    wide = heads * HK
    cols = pl.ds(pl.multiple_of(pl.program_id(0) * wide, wide), wide)
    total = against(refs[:2], refs[2:-1], cols).astype(BF16)
    for n in range(heads):
        out_ref[:, n, 0] = total[:, n * HK : (n + 1) * HK].reshape(seqs, local_len, HK)


def project_heads(normed, stacks, seqs, local_len):
    block = (seqs, 2, 1, local_len, HK)
    return pl.pallas_call(
        project_kernel,
        grid=(HEADS,),
        in_specs=[vmem_spec()] * (2 + len(stacks)),
        out_specs=pl.BlockSpec(block, lambda j: (0, j % 2, j // 2, 0, 0)),
        out_shape=pltpu.HBM((seqs, HEADS, 2, local_len, HK), BF16),
        compiler_params=limit(8),
        name="project",
    )(*normed, *stacks)


def pair_masks():
    row = lax.broadcasted_iota(jnp.int32, (PAIR, PAIR), 0)
    col = lax.broadcasted_iota(jnp.int32, (PAIR, PAIR), 1)
    causal = (row >= col) & ((row < CHUNK) == (col < CHUNK))
    return causal, row < CHUNK, col < CHUNK


def keys_and_total(f, gap, ones):
    keys = gap * sigmoid(-f)
    decay = jnp.log1p(-keys)
    high = decay.astype(BF16)
    low = (decay - high.astype(F32)).astype(BF16)
    return keys, dot(ones, high) + dot(ones, low)


def parts_of(a):
    high = a.astype(BF16).astype(F32)
    middle = (a - high).astype(BF16).astype(F32)
    return high, middle, a - high - middle


def state_kernel(head_ref, fv_ref, extra_ref, bound_ref, state_ref, out_ref, carry_ref):
    chunks = out_ref.shape[0]
    causal, first_row, first_col = pair_masks()
    ones = causal.astype(F32).astype(BF16)
    gap = 1.0 - bound_ref[:, pl.ds(pl.multiple_of(head_ref[0] * HK, HK), HK)]
    tail_row = lax.broadcasted_iota(jnp.int32, (TAIL, HK), 0)
    block = pl.program_id(0)

    @pl.when(block == 0)
    def _():
        carry_ref[...] = state_ref[0].T

    state = carry_ref[...]
    for p in range(chunks // 2):
        b = block * chunks + 2 * p
        f = fv_ref[pl.ds(b, 2), 0].reshape(PAIR, HK).astype(F32)
        keys, total = keys_and_total(f, gap, ones)
        lanes = pl.ds(pl.multiple_of(b * CHUNK, PAIR), PAIR)
        extra = jnp.broadcast_to(extra_ref[:, lanes], (PAIR, PAIR))
        run_rows = sum(dot_nt(part.astype(BF16), ones) for part in parts_of(extra))
        run = run_rows.T
        ends = [total[n * CHUNK + CHUNK - 1 : (n + 1) * CHUNK, :] for n in range(2)]
        run_ends = [run[n * CHUNK + CHUNK - 1 : (n + 1) * CHUNK, :] for n in range(2)]
        end = jnp.where(first_row, ends[0], ends[1])
        run_end = jnp.where(first_row, run_ends[0], run_ends[1])
        weighted = (keys * jnp.exp((end - total) + (run_end - run))).astype(BF16)
        own = run_rows[0:TAIL, :]
        turned = pltpu.roll(own, CHUNK, 1)
        first_lane = first_col[0:TAIL, :]
        for n in range(2):
            both = jnp.where(first_lane, own, turned) if n == 0 else jnp.where(first_lane, turned, own)
            high, middle, low = parts_of(both)
            tail = jnp.where(tail_row == 0, high, jnp.where(tail_row == 1, middle, low))
            out_ref[2 * p + n, 0:HV, :] = state.astype(BF16)
            out_ref[2 * p + n, HV:, :] = tail.astype(BF16)
            rows = slice(n * CHUNK, (n + 1) * CHUNK)
            added = dot_tn(fv_ref[b + n, 1], weighted[rows])
            state = state * jnp.exp(ends[n] + run_ends[n]) + added
    carry_ref[...] = state


def chunk_states(fv, extra, bound, state, head):
    chunks = fv.shape[0]
    group = 8
    return pl.pallas_call(
        state_kernel,
        grid=(chunks // group,),
        in_specs=[
            pl.BlockSpec(memory_space=pltpu.SMEM),
            vmem_spec(),
            pl.BlockSpec(extra.shape, lambda i: (0, 0)),
            pl.BlockSpec(bound.shape, lambda i: (0, 0)),
            pl.BlockSpec(state.shape, lambda i: (0, 0, 0)),
        ],
        out_specs=pl.BlockSpec((group, HV + TAIL, HK), lambda i: (i, 0, 0)),
        out_shape=pltpu.HBM((chunks, HV + TAIL, HK), BF16),
        scratch_shapes=[pltpu.VMEM((HV, HK), F32)],
        compiler_params=limit(6),
        name="state",
    )(head, fv, in_hbm(extra), in_hbm(bound), in_hbm(state))


def local_kernel(fv_ref, bound_ref, *refs):
    out_ref, a_refs, stacks = refs[-1], refs[:2], refs[2:-1]
    seqs, heads, _, _, _ = fv_ref.shape
    wide = heads * HK
    causal, _, _ = pair_masks()
    ones = causal.astype(F32).astype(BF16)
    q_pre = against(a_refs, stacks, slice(0, wide)).astype(BF16)
    g_pre = against(a_refs, stacks, slice(wide, 2 * wide)).astype(BF16)
    for p in range(seqs // 2):
        for h in range(heads):
            q = q_pre[p * PAIR : (p + 1) * PAIR, h * HK : (h + 1) * HK].astype(F32)
            f = fv_ref[2 * p : 2 * p + 2, h, 0].reshape(PAIR, HK).astype(F32)
            keys, total = keys_and_total(f, 1.0 - bound_ref[:, h * HK : (h + 1) * HK], ones)
            q_scaled = (q * sigmoid(q) * jnp.exp(total)).astype(BF16)
            k_scaled = (keys * jnp.exp(-total)).astype(BF16)
            out_ref[0, p, h] = q_scaled
            out_ref[1, p, h] = jnp.where(causal, dot_nt(q_scaled, k_scaled), 0.0).astype(BF16)
            out_ref[2, p, h] = g_pre[p * PAIR : (p + 1) * PAIR, h * HV : (h + 1) * HV]


def weight_kernel(where_ref, *refs):
    weight_ref = refs[-1]
    j = 0
    for stack in refs[:-1]:
        for first in range(0, stack.shape[0], ROWS):
            start = pl.multiple_of(place(where_ref, j) * OUT_ROWS, OUT_ROWS)
            for n in range(ROWS // OUT_ROWS):
                rows = slice(first + n * OUT_ROWS, first + (n + 1) * OUT_ROWS)
                weight_ref[pl.ds(start, OUT_ROWS), n * WIDE : (n + 1) * WIDE] = stack[rows, 2 * WIDE :]
            j += 1


def local_parts(normed, stacks, fv, bound):
    seqs, heads, _, _, _ = fv.shape
    return pl.pallas_call(
        local_kernel,
        in_specs=[vmem_spec()] * (4 + len(stacks)),
        out_shape=pltpu.HBM((3, seqs // 2, heads, PAIR, HK), BF16),
        compiler_params=limit(14),
        name="local",
    )(fv, bound, *normed, *stacks)


def out_weight(where, stacks, width):
    return pl.pallas_call(
        weight_kernel,
        in_specs=[pl.BlockSpec(memory_space=pltpu.SMEM)] + [vmem_spec()] * len(stacks),
        out_specs=vmem_spec(),
        out_shape=jax.ShapeDtypeStruct((WIDE, width), BF16),
        compiler_params=limit(4),
        name="weight",
    )(where, *stacks)


def output_kernel(state_ref, part_ref, fv_ref, weight_ref, norm_ref, post_ref, out_ref):
    heads = fv_ref.shape[1]
    pairs = out_ref.shape[0] // 2
    _, _, first_col = pair_masks()
    gain = norm_ref[...]
    rows = []
    for n_pair in range(pairs):
        p = n_pair
        gated = []
        for h in range(heads):
            runs, carried = [], []
            for n in range(2):
                s = pl.program_id(0) * 2 * pairs + 2 * p + n
                tail = state_ref[s, h, HV:, :].astype(F32)
                runs.append(tail[0:1, :] + tail[1:2, :] + tail[2:3, :])
                query = part_ref[0, p, h, n * CHUNK : (n + 1) * CHUNK, :]
                carried.append(dot_nt(query, state_ref[s, h, 0:HV, :]))
            run = jnp.where(first_col, runs[0], runs[1])
            run_cols = run.T
            weight = jnp.exp(jnp.minimum(run_cols - run, 0.0))
            scores = (part_ref[1, p, h].astype(F32) * weight).astype(BF16)
            v = fv_ref[2 * p : 2 * p + 2, h, 0].reshape(PAIR, HV)
            out = jnp.concatenate(carried, axis=0) * jnp.exp(run_cols) + dot(scores, v)
            scale = lax.rsqrt(jnp.mean(out * out, axis=-1, keepdims=True) + EPS)
            head = (out * scale * gain).astype(BF16).astype(F32)
            gate = part_ref[2, p, h].astype(F32)
            gated.append((head * (gate * sigmoid(gate))).astype(BF16))
        rows.append(jnp.concatenate(gated, axis=1))
    mixed = dot(jnp.concatenate(rows, axis=0), weight_ref[...])
    scale = lax.rsqrt(jnp.mean(mixed * mixed, axis=-1, keepdims=True) + EPS)
    out_ref[...] = (mixed * scale * post_ref[...]).astype(BF16).reshape(out_ref.shape)


def output_rows(states, parts, fv, weight, norm_gain, post_gain):
    seqs, heads, _, local_len, _ = fv.shape
    width = weight.shape[1]
    group = 4
    return pl.pallas_call(
        output_kernel,
        grid=(seqs // group,),
        in_specs=[
            vmem_spec(),
            pl.BlockSpec((3, group // 2, heads, PAIR, HK), lambda i: (0, i, 0, 0, 0)),
            pl.BlockSpec((group, heads, 1, local_len, HK), lambda i: (i, 0, 1, 0, 0)),
            vmem_spec(),
            vmem_spec(),
            vmem_spec(),
        ],
        out_specs=pl.BlockSpec((group, local_len, width), lambda i: (i, 0, 0)),
        out_shape=jax.ShapeDtypeStruct((seqs, local_len, width), BF16),
        compiler_params=limit(12),
        name="output",
    )(states, in_hbm(parts), in_hbm(fv), weight, norm_gain.reshape(1, HV), post_gain.reshape(1, width))


def layer(
    tokens,
    pre_gain,
    w_query,
    w_forget,
    w_value,
    w_gate,
    lower_bound,
    extra_decay,
    initial_state,
    norm_gain,
    w_out,
    post_gain,
):
    seqs, local_len, width = tokens.shape
    items = seqs * HEADS
    where = jnp.stack([lax.axis_index("y"), lax.axis_index("c")]).astype(jnp.int32)
    bound = lower_bound.reshape(1, HEADS * HK)
    head = lax.axis_index("x").astype(jnp.int32).reshape(1)

    first = joined((w_forget, w_value), ((0, (0, 0), (0, 0)), (1, (0, 0), (0, WIDE))), 2 * WIDE)
    places = [(0, (0, 0), (0, 0)), (1, (0, 0), (0, WIDE))]
    places += [(2, (0, n * WIDE), (n * OUT_ROWS, 2 * WIDE)) for n in range(width // WIDE)]
    second = joined((w_query, w_gate, w_out), tuple(places), 3 * WIDE)
    rows = tokens.reshape(seqs * local_len, width)
    normed = [normed_tokens(rows, pre_gain, where, half) for half in range(2)]

    first_own, first_other = gathered_y(first, ((), normed[:1], normed[1:], (second,)), True)
    fv = project_heads(normed, first_own + first_other, seqs, local_len)
    moved = lax.all_to_all(fv.reshape(items, 2 * local_len, HK), SP, 0, 0, tiled=True)
    moved = moved.reshape(items, 2, local_len, HK)
    starts = chunk_states(moved, extra_decay, bound, initial_state, head)
    states = lax.all_to_all(starts, SP, 0, 0, tiled=True)

    second_own, second_other = gathered_y(second, ((), (), (), ()), False)
    stacks = second_own + second_other
    parts = local_parts(normed, stacks, fv, bound)
    weight = out_weight(where, stacks, width)
    states = states.reshape(seqs, HEADS, HV + TAIL, HK)
    return output_rows(states, parts, fv, weight, norm_gain, post_gain)


def solution(mesh):
    split = Mesh(mesh.devices.reshape(8, 4, 8, 2), ("z", "x", "y", "c"))
    in_specs = (
        P(DP, SP, None),
        P(),
        P(DP, None),
        P(DP, None),
        P(DP, None),
        P(DP, None),
        P(),
        P(DP_SP, None),
        P(DP_SP, None, None),
        P(),
        P(DP, None),
        P(),
    )
    out_specs = P(DP, SP, None)
    return jax.shard_map(layer, mesh=split, in_specs=in_specs, out_specs=out_specs, check_vma=False)
```

```python
import functools

import jax
import jax.numpy as jnp
from jax import lax
from jax.experimental import pallas as pl
from jax.experimental.pallas import tpu as pltpu
from jax.sharding import Mesh
from jax.sharding import PartitionSpec as P


HEADS = 4
HK = 128
HV = 128
CHUNK = 64
PAIR = 2 * CHUNK
TAIL = 8
SP = ("z", "x")
DP = ("y", "c")
DP_SP = ("y", "c", "z", "x")
OFFSETS = (0, -1, 1, -2, 2, -3, 3, 4)
ROWS = 128
OUT_ROWS = 32
EPS = 1e-06
WIDE = HEADS * HV


F32 = jnp.float32
BF16 = jnp.bfloat16


def shifted(a, step):
    size = lax.axis_size("y")
    return lax.ppermute(a, "y", [(i, (i + step) % size) for i in range(size)])


def swapped(a):
    return lax.ppermute(a, "c", [(0, 1), (1, 0)])


def after(values, others):
    return lax.optimization_barrier((*values, *others))[: len(values)]


def gathered_y(shard, waits, halves, cut):
    pieces = [shard]
    own, other = [], []
    up = down = shard
    for k in range(4):
        up, down = after((up, down), waits[k]) if waits[k] else (up, down)
        if k == 3 and halves:
            middle = shard.shape[0] // 2
            up, down = up[:middle], down[middle:]
        up = shifted(up, 1)
        if k < 3 or halves:
            down = shifted(down, -1)
        if k == 2:
            own.append(stacked_pieces(pieces[:cut]))
            other.append(swapped(own[-1]))
            pieces = pieces[cut:]
        pieces += [up, down] if k < 3 or halves else [up]
    own.append(stacked_pieces(pieces))
    other.append(swapped(own[-1]))
    return own, other


def in_hbm(a):
    return pltpu.with_memory_space_constraint(a, pltpu.HBM)


def join_kernel(*refs, places):
    out_ref, sems = refs[-2:]
    copies = []
    for n, (k, (rows, cols), (r, c)) in enumerate(places):
        source = refs[k].at[:, pl.ds(cols, WIDE)]
        target = out_ref.at[pl.ds(r, source.shape[0]), pl.ds(c, WIDE)]
        copies.append(pltpu.make_async_copy(source, target, sems.at[n]))
    for copy in copies:
        copy.start()
    for copy in copies:
        copy.wait()


def joined(arrays, places, width):
    return pl.pallas_call(
        functools.partial(join_kernel, places=places),
        in_specs=[pl.BlockSpec(memory_space=pl.ANY)] * len(arrays),
        out_specs=vmem_spec(),
        out_shape=jax.ShapeDtypeStruct((ROWS, width), BF16),
        scratch_shapes=[pltpu.SemaphoreType.DMA((len(places),))],
        compiler_params=limit(2),
    )(*[in_hbm(a) for a in arrays])


def stack_kernel(*refs):
    out_ref = refs[-1]
    first = 0
    for ref in refs[:-1]:
        rows = ref.shape[0]
        out_ref[first : first + rows, :] = ref[...]
        first += rows


def stacked_pieces(pieces):
    rows = sum(p.shape[0] for p in pieces)
    return pl.pallas_call(
        stack_kernel,
        in_specs=[vmem_spec()] * len(pieces),
        out_specs=vmem_spec(),
        out_shape=jax.ShapeDtypeStruct((rows, pieces[0].shape[1]), BF16),
        compiler_params=limit(6),
        name="stack",
    )(*pieces)


def against(a_ref, refs, cols):
    total = None
    first = 0
    for ref in refs:
        rows = ref.shape[0]
        part = dot(a_ref[:, first : first + rows], ref[:, cols])
        total = part if total is None else total + part
        first += rows
    return total


def dot(a, b):
    return jnp.dot(a, b, preferred_element_type=F32)


def dot_nt(a, b):
    return lax.dot_general(a, b, (((1,), (1,)), ((), ())), preferred_element_type=F32)


def dot_tn(a, b):
    return lax.dot_general(a, b, (((0,), (0,)), ((), ())), preferred_element_type=F32)


def sigmoid(a):
    return 0.5 * jnp.tanh(0.5 * a) + 0.5


def place(where_ref, j):
    core = where_ref[1] if j < len(OFFSETS) else 1 - where_ref[1]
    return 2 * ((where_ref[0] + OFFSETS[j % len(OFFSETS)] + 8) & 7) + core


def norm_kernel(where_ref, x_ref, gain_ref, out_ref, held_ref, sems):
    tile = held_ref.shape[0] // sems.shape[0]
    copies = []
    for n in range(sems.shape[0]):
        rows = pl.ds(n * tile, tile)
        copies.append(pltpu.make_async_copy(x_ref.at[rows], held_ref.at[rows], sems.at[n]))
        copies[-1].start()
    for n, copy in enumerate(copies):
        copy.wait()
        rows = slice(n * tile, (n + 1) * tile)
        x = held_ref[rows, :].astype(F32)
        scale = lax.rsqrt(jnp.mean(x * x, axis=-1, keepdims=True) + EPS)
        for j in range(2 * len(OFFSETS)):
            cols = pl.ds(pl.multiple_of(place(where_ref, j) * ROWS, ROWS), ROWS)
            part = held_ref[rows, cols].astype(F32) * scale * gain_ref[:, cols]
            out_ref[rows, j * ROWS : (j + 1) * ROWS] = part.astype(BF16)


def normed_tokens(tokens, pre_gain, where):
    rows, width = tokens.shape
    return pl.pallas_call(
        norm_kernel,
        in_specs=[
            pl.BlockSpec(memory_space=pltpu.SMEM),
            pl.BlockSpec(memory_space=pl.ANY),
            vmem_spec(),
        ],
        out_specs=vmem_spec(),
        out_shape=jax.ShapeDtypeStruct((rows, width), BF16),
        scratch_shapes=[pltpu.VMEM((rows, width), BF16), pltpu.SemaphoreType.DMA((4,))],
        compiler_params=limit(6),
        name="norm",
    )(where, in_hbm(tokens), in_hbm(pre_gain.reshape(1, width)))


def vmem_spec():
    return pl.BlockSpec(memory_space=pltpu.VMEM)


def limit(mib):
    return pltpu.CompilerParams(vmem_limit_bytes=mib << 20)


def project_kernel(where_ref, a_ref, *refs):
    out_ref, weight_ref = refs[-2:]
    stacks = refs[:-2]
    seqs, heads, _, local_len, _ = out_ref.shape
    wide = heads * HK
    step = pl.program_id(0)
    cols = pl.ds(pl.multiple_of(step * wide, wide), wide)
    total = against(a_ref, stacks, cols).astype(BF16)
    for n in range(heads):
        out_ref[:, n, 0] = total[:, n * HK : (n + 1) * HK].reshape(seqs, local_len, HK)
    j = 0
    for stack in stacks:
        for first in range(0, stack.shape[0], ROWS):
            start = pl.multiple_of(place(where_ref, j) * OUT_ROWS, OUT_ROWS)
            rows = pl.ds(pl.multiple_of(first + step * OUT_ROWS, OUT_ROWS), OUT_ROWS)
            weight_ref[pl.ds(start, OUT_ROWS), :] = stack[rows, 2 * WIDE :]
            j += 1


def project_heads(where, normed, stacks, seqs, local_len, width):
    block = (seqs, 2, 1, local_len, HK)
    return pl.pallas_call(
        project_kernel,
        grid=(HEADS,),
        in_specs=[pl.BlockSpec(memory_space=pltpu.SMEM)] + [vmem_spec()] * (1 + len(stacks)),
        out_specs=(
            pl.BlockSpec(block, lambda j: (0, j % 2, j // 2, 0, 0)),
            pl.BlockSpec((WIDE, WIDE), lambda j: (0, j)),
        ),
        out_shape=(
            pltpu.HBM((seqs, HEADS, 2, local_len, HK), BF16),
            pltpu.HBM((WIDE, width), BF16),
        ),
        compiler_params=limit(8),
        name="project",
    )(where, normed, *stacks)


def pair_masks():
    row = lax.broadcasted_iota(jnp.int32, (PAIR, PAIR), 0)
    col = lax.broadcasted_iota(jnp.int32, (PAIR, PAIR), 1)
    causal = (row >= col) & ((row < CHUNK) == (col < CHUNK))
    return causal, row < CHUNK, col < CHUNK


def keys_and_total(f, gap, ones):
    keys = gap * sigmoid(-f)
    decay = jnp.log1p(-keys)
    high = decay.astype(BF16)
    low = (decay - high.astype(F32)).astype(BF16)
    return keys, dot(ones, high) + dot(ones, low)


def parts_of(a):
    high = a.astype(BF16).astype(F32)
    middle = (a - high).astype(BF16).astype(F32)
    return high, middle, a - high - middle


def state_kernel(head_ref, fv_ref, extra_ref, bound_ref, state_ref, out_ref, carry_ref, run_ref):
    chunks = out_ref.shape[0]
    causal, first_row, first_col = pair_masks()
    ones = causal.astype(F32).astype(BF16)
    gap = 1.0 - bound_ref[:, pl.ds(pl.multiple_of(head_ref[0] * HK, HK), HK)]
    tail_row = lax.broadcasted_iota(jnp.int32, (TAIL, HK), 0)
    block = pl.program_id(0)

    @pl.when(block == 0)
    def _():
        carry_ref[...] = state_ref[0].T
        for p in range(run_ref.shape[0]):
            run_ref[p : p + 1, :] = extra_ref[:, p * PAIR : (p + 1) * PAIR]
        split = [part.astype(BF16) for part in parts_of(run_ref[...])]
        run_ref[...] = sum(dot_nt(part, ones) for part in split)

    state = carry_ref[...]
    for p in range(chunks // 2):
        b = block * chunks + 2 * p
        f = fv_ref[pl.ds(b, 2), 0].reshape(PAIR, HK).astype(F32)
        keys, total = keys_and_total(f, gap, ones)
        run_row = run_ref[pl.ds(block * (chunks // 2) + p, 1), :]
        run = jnp.broadcast_to(run_row, (PAIR, PAIR)).T
        ends = [total[n * CHUNK + CHUNK - 1 : (n + 1) * CHUNK, :] for n in range(2)]
        run_ends = [run[n * CHUNK + CHUNK - 1 : (n + 1) * CHUNK, :] for n in range(2)]
        end = jnp.where(first_row, ends[0], ends[1])
        run_end = jnp.where(first_row, run_ends[0], run_ends[1])
        weighted = (keys * jnp.exp((end - total) + (run_end - run))).astype(BF16)
        own = jnp.broadcast_to(run_row, (TAIL, PAIR))
        turned = pltpu.roll(own, CHUNK, 1)
        first_lane = first_col[0:TAIL, :]
        for n in range(2):
            both = jnp.where(first_lane, own, turned) if n == 0 else jnp.where(first_lane, turned, own)
            high, middle, low = parts_of(both)
            tail = jnp.where(tail_row == 0, high, jnp.where(tail_row == 1, middle, low))
            out_ref[2 * p + n, 0:HV, :] = state.astype(BF16)
            out_ref[2 * p + n, HV:, :] = tail.astype(BF16)
            rows = slice(n * CHUNK, (n + 1) * CHUNK)
            added = dot_tn(fv_ref[b + n, 1], weighted[rows])
            state = state * jnp.exp(ends[n] + run_ends[n]) + added
    carry_ref[...] = state


def chunk_states(fv, extra, bound, state, head):
    chunks = fv.shape[0]
    group = 8
    return pl.pallas_call(
        state_kernel,
        grid=(chunks // group,),
        in_specs=[
            pl.BlockSpec(memory_space=pltpu.SMEM),
            vmem_spec(),
            pl.BlockSpec(extra.shape, lambda i: (0, 0)),
            pl.BlockSpec(bound.shape, lambda i: (0, 0)),
            pl.BlockSpec(state.shape, lambda i: (0, 0, 0)),
        ],
        out_specs=pl.BlockSpec((group, HV + TAIL, HK), lambda i: (i, 0, 0)),
        out_shape=pltpu.HBM((chunks, HV + TAIL, HK), BF16),
        scratch_shapes=[pltpu.VMEM((HV, HK), F32), pltpu.VMEM((chunks // 2, PAIR), F32)],
        compiler_params=limit(6),
        name="state",
    )(head, fv, in_hbm(extra), in_hbm(bound), in_hbm(state))


def local_kernel(a_ref, fv_ref, bound_ref, *refs):
    out_ref, stacks = refs[-1], refs[:-1]
    seqs, heads, _, _, _ = fv_ref.shape
    wide = heads * HK
    causal, _, _ = pair_masks()
    ones = causal.astype(F32).astype(BF16)
    q_pre = against(a_ref, stacks, slice(0, wide)).astype(BF16)
    g_pre = against(a_ref, stacks, slice(wide, 2 * wide)).astype(BF16)
    for p in range(seqs // 2):
        for h in range(heads):
            q = q_pre[p * PAIR : (p + 1) * PAIR, h * HK : (h + 1) * HK].astype(F32)
            f = fv_ref[2 * p : 2 * p + 2, h, 0].reshape(PAIR, HK).astype(F32)
            keys, total = keys_and_total(f, 1.0 - bound_ref[:, h * HK : (h + 1) * HK], ones)
            q_scaled = (q * sigmoid(q) * jnp.exp(total)).astype(BF16)
            k_scaled = (keys * jnp.exp(-total)).astype(BF16)
            out_ref[0, p, h] = q_scaled
            out_ref[1, p, h] = jnp.where(causal, dot_nt(q_scaled, k_scaled), 0.0).astype(BF16)
            out_ref[2, p, h] = g_pre[p * PAIR : (p + 1) * PAIR, h * HV : (h + 1) * HV]


def local_parts(normed, stacks, fv, bound):
    seqs, heads, _, _, _ = fv.shape
    return pl.pallas_call(
        local_kernel,
        in_specs=[vmem_spec()] * (3 + len(stacks)),
        out_shape=pltpu.HBM((3, seqs // 2, heads, PAIR, HK), BF16),
        compiler_params=limit(14),
        name="local",
    )(normed, fv, bound, *stacks)


def output_kernel(
    state_ref, part_ref, fv_ref, weight_ref, norm_ref, post_ref, out_ref, held_ref, sem
):
    heads = fv_ref.shape[1]
    pairs = out_ref.shape[0] // 2
    _, _, first_col = pair_masks()
    gain = norm_ref[...]
    copy = pltpu.make_async_copy(weight_ref, held_ref, sem)

    @pl.when(pl.program_id(0) == 0)
    def _():
        copy.start()

    rows = []
    for n_pair in range(pairs):
        p = n_pair
        gated = []
        for h in range(heads):
            runs, carried = [], []
            for n in range(2):
                s = pl.program_id(0) * 2 * pairs + 2 * p + n
                tail = state_ref[s, h, HV:, :].astype(F32)
                runs.append(tail[0:1, :] + tail[1:2, :] + tail[2:3, :])
                query = part_ref[0, p, h, n * CHUNK : (n + 1) * CHUNK, :]
                carried.append(dot_nt(query, state_ref[s, h, 0:HV, :]))
            run = jnp.where(first_col, runs[0], runs[1])
            run_cols = run.T
            weight = jnp.exp(jnp.minimum(run_cols - run, 0.0))
            scores = (part_ref[1, p, h].astype(F32) * weight).astype(BF16)
            v = fv_ref[2 * p : 2 * p + 2, h, 0].reshape(PAIR, HV)
            out = jnp.concatenate(carried, axis=0) * jnp.exp(run_cols) + dot(scores, v)
            scale = lax.rsqrt(jnp.mean(out * out, axis=-1, keepdims=True) + EPS)
            head = (out * scale * gain).astype(BF16).astype(F32)
            gate = part_ref[2, p, h].astype(F32)
            gated.append((head * (gate * sigmoid(gate))).astype(BF16))
        rows.append(jnp.concatenate(gated, axis=1))

    @pl.when(pl.program_id(0) == 0)
    def _():
        copy.wait()

    mixed = dot(jnp.concatenate(rows, axis=0), held_ref[...])
    scale = lax.rsqrt(jnp.mean(mixed * mixed, axis=-1, keepdims=True) + EPS)
    out_ref[...] = (mixed * scale * post_ref[...]).astype(BF16).reshape(out_ref.shape)


def output_rows(states, parts, fv, weight, norm_gain, post_gain):
    seqs, heads, _, local_len, _ = fv.shape
    width = weight.shape[1]
    group = 4
    return pl.pallas_call(
        output_kernel,
        grid=(seqs // group,),
        in_specs=[
            vmem_spec(),
            pl.BlockSpec((3, group // 2, heads, PAIR, HK), lambda i: (0, i, 0, 0, 0)),
            pl.BlockSpec((group, heads, 1, local_len, HK), lambda i: (i, 0, 1, 0, 0)),
            pl.BlockSpec(memory_space=pl.ANY),
            vmem_spec(),
            vmem_spec(),
        ],
        out_specs=pl.BlockSpec((group, local_len, width), lambda i: (i, 0, 0)),
        out_shape=jax.ShapeDtypeStruct((seqs, local_len, width), BF16),
        scratch_shapes=[pltpu.VMEM(weight.shape, BF16), pltpu.SemaphoreType.DMA(())],
        compiler_params=limit(12),
        name="output",
    )(states, in_hbm(parts), in_hbm(fv), in_hbm(weight), norm_gain.reshape(1, HV), post_gain.reshape(1, width))


def layer(
    tokens,
    pre_gain,
    w_query,
    w_forget,
    w_value,
    w_gate,
    lower_bound,
    extra_decay,
    initial_state,
    norm_gain,
    w_out,
    post_gain,
):
    seqs, local_len, width = tokens.shape
    items = seqs * HEADS
    where = jnp.stack([lax.axis_index("y"), lax.axis_index("c")]).astype(jnp.int32)
    bound = lower_bound.reshape(1, HEADS * HK)
    head = lax.axis_index("x").astype(jnp.int32).reshape(1)

    places = [(0, (0, 0), (0, 0)), (1, (0, 0), (0, WIDE))]
    second = joined((w_query, w_gate), tuple(places), 2 * WIDE)
    places += [(2, (0, n * WIDE), (n * OUT_ROWS, 2 * WIDE)) for n in range(width // WIDE)]
    first = joined((w_forget, w_value, w_out), tuple(places), 3 * WIDE)
    rows = tokens.reshape(seqs * local_len, width)
    normed = normed_tokens(rows, pre_gain, where)

    first_own, first_other = gathered_y(first, ((), (normed,), (second,), ()), True, 5)
    fv, weight = project_heads(where, normed, first_own + first_other, seqs, local_len, width)
    moved = lax.all_to_all(fv.reshape(items, 2 * local_len, HK), SP, 0, 0, tiled=True)
    moved = moved.reshape(items, 2, local_len, HK)
    starts = chunk_states(moved, extra_decay, bound, initial_state, head)
    states = lax.all_to_all(starts, SP, 0, 0, tiled=True)

    second_own, second_other = gathered_y(second, ((), (), (), ()), False, 4)
    stacks = second_own + second_other
    parts = local_parts(normed, stacks, fv, bound)
    states = states.reshape(seqs, HEADS, HV + TAIL, HK)
    return output_rows(states, parts, fv, weight, norm_gain, post_gain)


def solution(mesh):
    split = Mesh(mesh.devices.reshape(8, 4, 8, 2), ("z", "x", "y", "c"))
    in_specs = (
        P(DP, SP, None),
        P(),
        P(DP, None),
        P(DP, None),
        P(DP, None),
        P(DP, None),
        P(),
        P(DP_SP, None),
        P(DP_SP, None, None),
        P(),
        P(DP, None),
        P(),
    )
    out_specs = P(DP, SP, None)
    return jax.shard_map(layer, mesh=split, in_specs=in_specs, out_specs=out_specs, check_vma=False)
```

```python
import functools

import jax
import jax.numpy as jnp
from jax import lax
from jax.experimental import pallas as pl
from jax.experimental.pallas import tpu as pltpu
from jax.sharding import Mesh
from jax.sharding import PartitionSpec as P


HEADS = 4
HK = 128
HV = 128
CHUNK = 64
PAIR = 2 * CHUNK
TAIL = 8
SP = ("z", "x")
DP = ("y", "c")
DP_SP = ("y", "c", "z", "x")
OFFSETS = (0, -1, 1, -2, 2, -3, 3, 4)
ROWS = 128
OUT_ROWS = 32
EPS = 1e-06
WIDE = HEADS * HV


F32 = jnp.float32
BF16 = jnp.bfloat16


def shifted(a, step):
    size = lax.axis_size("y")
    return lax.ppermute(a, "y", [(i, (i + step) % size) for i in range(size)])


def swapped(a):
    return lax.ppermute(a, "c", [(0, 1), (1, 0)])


def after(values, others):
    return lax.optimization_barrier((*values, *others))[: len(values)]


def gathered_y(shard, waits, halves, cut):
    pieces = [shard]
    own, other = [], []
    up = down = shard
    for k in range(4):
        up = after((up,), waits[k])[0] if waits[k] else up
        if k == 3 and halves:
            middle = shard.shape[0] // 2
            up, down = up[:middle], down[middle:]
        up = shifted(up, 1)
        if k < 3 or halves:
            down = shifted(down, -1)
        if k == 2:
            own.append(stacked_pieces(pieces[:cut]))
            other.append(swapped(own[-1]))
            pieces = pieces[cut:]
        pieces += [up, down] if k < 3 or halves else [up]
    own.append(stacked_pieces(pieces))
    other.append(swapped(own[-1]))
    return own, other


def in_hbm(a):
    return pltpu.with_memory_space_constraint(a, pltpu.HBM)


def join_kernel(*refs, places):
    out_ref, sems = refs[-2:]
    copies = []
    for n, (k, (rows, cols), (r, c)) in enumerate(places):
        source = refs[k].at[:, pl.ds(cols, WIDE)]
        target = out_ref.at[pl.ds(r, source.shape[0]), pl.ds(c, WIDE)]
        copies.append(pltpu.make_async_copy(source, target, sems.at[n]))
    for copy in copies:
        copy.start()
    for copy in copies:
        copy.wait()


def joined(arrays, places, width):
    return pl.pallas_call(
        functools.partial(join_kernel, places=places),
        in_specs=[pl.BlockSpec(memory_space=pl.ANY)] * len(arrays),
        out_specs=vmem_spec(),
        out_shape=jax.ShapeDtypeStruct((ROWS, width), BF16),
        scratch_shapes=[pltpu.SemaphoreType.DMA((len(places),))],
        compiler_params=limit(2),
    )(*[in_hbm(a) for a in arrays])


def stack_kernel(*refs):
    out_ref = refs[-1]
    first = 0
    for ref in refs[:-1]:
        rows = ref.shape[0]
        out_ref[first : first + rows, :] = ref[...]
        first += rows


def stacked_pieces(pieces):
    rows = sum(p.shape[0] for p in pieces)
    return pl.pallas_call(
        stack_kernel,
        in_specs=[vmem_spec()] * len(pieces),
        out_specs=vmem_spec(),
        out_shape=jax.ShapeDtypeStruct((rows, pieces[0].shape[1]), BF16),
        compiler_params=limit(6),
        name="stack",
    )(*pieces)


def against(a_ref, refs, cols):
    total = None
    first = 0
    for ref in refs:
        rows = ref.shape[0]
        part = dot(a_ref[:, first : first + rows], ref[:, cols])
        total = part if total is None else total + part
        first += rows
    return total


def dot(a, b):
    return jnp.dot(a, b, preferred_element_type=F32)


def dot_nt(a, b):
    return lax.dot_general(a, b, (((1,), (1,)), ((), ())), preferred_element_type=F32)


def dot_tn(a, b):
    return lax.dot_general(a, b, (((0,), (0,)), ((), ())), preferred_element_type=F32)


def sigmoid(a):
    return 0.5 * jnp.tanh(0.5 * a) + 0.5


def place(where_ref, j):
    core = where_ref[1] if j < len(OFFSETS) else 1 - where_ref[1]
    return 2 * ((where_ref[0] + OFFSETS[j % len(OFFSETS)] + 8) & 7) + core


def norm_kernel(where_ref, x_ref, gain_ref, out_ref, held_ref, sems):
    tile = held_ref.shape[0] // sems.shape[0]
    copies = []
    for n in range(sems.shape[0]):
        rows = pl.ds(n * tile, tile)
        copies.append(pltpu.make_async_copy(x_ref.at[rows], held_ref.at[rows], sems.at[n]))
        copies[-1].start()
    for n, copy in enumerate(copies):
        copy.wait()
        rows = slice(n * tile, (n + 1) * tile)
        x = held_ref[rows, :].astype(F32)
        scale = lax.rsqrt(jnp.mean(x * x, axis=-1, keepdims=True) + EPS)
        for j in range(2 * len(OFFSETS)):
            cols = pl.ds(pl.multiple_of(place(where_ref, j) * ROWS, ROWS), ROWS)
            part = held_ref[rows, cols].astype(F32) * scale * gain_ref[:, cols]
            out_ref[rows, j * ROWS : (j + 1) * ROWS] = part.astype(BF16)


def normed_tokens(tokens, pre_gain, where):
    rows, width = tokens.shape
    return pl.pallas_call(
        norm_kernel,
        in_specs=[
            pl.BlockSpec(memory_space=pltpu.SMEM),
            pl.BlockSpec(memory_space=pl.ANY),
            vmem_spec(),
        ],
        out_specs=vmem_spec(),
        out_shape=jax.ShapeDtypeStruct((rows, width), BF16),
        scratch_shapes=[pltpu.VMEM((rows, width), BF16), pltpu.SemaphoreType.DMA((4,))],
        compiler_params=limit(6),
        name="norm",
    )(where, in_hbm(tokens), in_hbm(pre_gain.reshape(1, width)))


def vmem_spec():
    return pl.BlockSpec(memory_space=pltpu.VMEM)


def limit(mib):
    return pltpu.CompilerParams(vmem_limit_bytes=mib << 20)


def project_kernel(a_ref, *refs):
    out_ref = refs[-1]
    seqs, heads, _, local_len, _ = out_ref.shape
    wide = heads * HK
    cols = pl.ds(pl.multiple_of(pl.program_id(0) * wide, wide), wide)
    total = against(a_ref, refs[:-1], cols).astype(BF16)
    for n in range(heads):
        out_ref[:, n, 0] = total[:, n * HK : (n + 1) * HK].reshape(seqs, local_len, HK)


def project_heads(normed, stacks, seqs, local_len):
    block = (seqs, 2, 1, local_len, HK)
    return pl.pallas_call(
        project_kernel,
        grid=(HEADS,),
        in_specs=[vmem_spec()] * (1 + len(stacks)),
        out_specs=pl.BlockSpec(block, lambda j: (0, j % 2, j // 2, 0, 0)),
        out_shape=pltpu.HBM((seqs, HEADS, 2, local_len, HK), BF16),
        compiler_params=limit(8),
        name="project",
    )(normed, *stacks)


def pair_masks():
    row = lax.broadcasted_iota(jnp.int32, (PAIR, PAIR), 0)
    col = lax.broadcasted_iota(jnp.int32, (PAIR, PAIR), 1)
    causal = (row >= col) & ((row < CHUNK) == (col < CHUNK))
    return causal, row < CHUNK, col < CHUNK


def keys_and_total(f, gap, ones):
    keys = gap * sigmoid(-f)
    decay = jnp.log1p(-keys)
    high = decay.astype(BF16)
    low = (decay - high.astype(F32)).astype(BF16)
    return keys, dot(ones, high) + dot(ones, low)


def parts_of(a):
    high = a.astype(BF16).astype(F32)
    middle = (a - high).astype(BF16).astype(F32)
    return high, middle, a - high - middle


def state_kernel(head_ref, fv_ref, extra_ref, bound_ref, state_ref, out_ref, carry_ref, run_ref):
    chunks = out_ref.shape[0]
    causal, first_row, first_col = pair_masks()
    ones = causal.astype(F32).astype(BF16)
    gap = 1.0 - bound_ref[:, pl.ds(pl.multiple_of(head_ref[0] * HK, HK), HK)]
    tail_row = lax.broadcasted_iota(jnp.int32, (TAIL, HK), 0)
    block = pl.program_id(0)

    @pl.when(block == 0)
    def _():
        carry_ref[...] = state_ref[0].T
        for p in range(run_ref.shape[0]):
            run_ref[p : p + 1, :] = extra_ref[:, p * PAIR : (p + 1) * PAIR]
        split = [part.astype(BF16) for part in parts_of(run_ref[...])]
        run_ref[...] = sum(dot_nt(part, ones) for part in split)

    state = carry_ref[...]
    for p in range(chunks // 2):
        b = block * chunks + 2 * p
        f = fv_ref[pl.ds(b, 2), 0].reshape(PAIR, HK).astype(F32)
        keys, total = keys_and_total(f, gap, ones)
        run_row = run_ref[pl.ds(block * (chunks // 2) + p, 1), :]
        run = jnp.broadcast_to(run_row, (PAIR, PAIR)).T
        ends = [total[n * CHUNK + CHUNK - 1 : (n + 1) * CHUNK, :] for n in range(2)]
        run_ends = [run[n * CHUNK + CHUNK - 1 : (n + 1) * CHUNK, :] for n in range(2)]
        end = jnp.where(first_row, ends[0], ends[1])
        run_end = jnp.where(first_row, run_ends[0], run_ends[1])
        weighted = (keys * jnp.exp((end - total) + (run_end - run))).astype(BF16)
        own = jnp.broadcast_to(run_row, (TAIL, PAIR))
        turned = pltpu.roll(own, CHUNK, 1)
        first_lane = first_col[0:TAIL, :]
        for n in range(2):
            both = jnp.where(first_lane, own, turned) if n == 0 else jnp.where(first_lane, turned, own)
            high, middle, low = parts_of(both)
            tail = jnp.where(tail_row == 0, high, jnp.where(tail_row == 1, middle, low))
            out_ref[2 * p + n, 0:HV, :] = state.astype(BF16)
            out_ref[2 * p + n, HV:, :] = tail.astype(BF16)
            rows = slice(n * CHUNK, (n + 1) * CHUNK)
            added = dot_tn(fv_ref[b + n, 1], weighted[rows])
            state = state * jnp.exp(ends[n] + run_ends[n]) + added
    carry_ref[...] = state


def chunk_states(fv, extra, bound, state, head):
    chunks = fv.shape[0]
    group = 8
    return pl.pallas_call(
        state_kernel,
        grid=(chunks // group,),
        in_specs=[
            pl.BlockSpec(memory_space=pltpu.SMEM),
            vmem_spec(),
            pl.BlockSpec(extra.shape, lambda i: (0, 0)),
            pl.BlockSpec(bound.shape, lambda i: (0, 0)),
            pl.BlockSpec(state.shape, lambda i: (0, 0, 0)),
        ],
        out_specs=pl.BlockSpec((group, HV + TAIL, HK), lambda i: (i, 0, 0)),
        out_shape=pltpu.HBM((chunks, HV + TAIL, HK), BF16),
        scratch_shapes=[pltpu.VMEM((HV, HK), F32), pltpu.VMEM((chunks // 2, PAIR), F32)],
        compiler_params=limit(6),
        name="state",
    )(head, fv, in_hbm(extra), in_hbm(bound), in_hbm(state))


def local_kernel(a_ref, fv_ref, bound_ref, *refs):
    out_ref, stacks = refs[-1], refs[:-1]
    seqs, heads, _, _, _ = fv_ref.shape
    wide = heads * HK
    causal, _, _ = pair_masks()
    ones = causal.astype(F32).astype(BF16)
    q_pre = against(a_ref, stacks, slice(0, wide)).astype(BF16)
    g_pre = against(a_ref, stacks, slice(wide, 2 * wide)).astype(BF16)
    for p in range(seqs // 2):
        for h in range(heads):
            q = q_pre[p * PAIR : (p + 1) * PAIR, h * HK : (h + 1) * HK].astype(F32)
            f = fv_ref[2 * p : 2 * p + 2, h, 0].reshape(PAIR, HK).astype(F32)
            keys, total = keys_and_total(f, 1.0 - bound_ref[:, h * HK : (h + 1) * HK], ones)
            q_scaled = (q * sigmoid(q) * jnp.exp(total)).astype(BF16)
            k_scaled = (keys * jnp.exp(-total)).astype(BF16)
            out_ref[0, p, h] = q_scaled
            out_ref[1, p, h] = jnp.where(causal, dot_nt(q_scaled, k_scaled), 0.0).astype(BF16)
            out_ref[2, p, h] = g_pre[p * PAIR : (p + 1) * PAIR, h * HV : (h + 1) * HV]


def weight_kernel(where_ref, *refs):
    weight_ref = refs[-1]
    j = 0
    for stack in refs[:-1]:
        for first in range(0, stack.shape[0], ROWS):
            start = pl.multiple_of(place(where_ref, j) * OUT_ROWS, OUT_ROWS)
            for n in range(ROWS // OUT_ROWS):
                rows = slice(first + n * OUT_ROWS, first + (n + 1) * OUT_ROWS)
                weight_ref[pl.ds(start, OUT_ROWS), n * WIDE : (n + 1) * WIDE] = stack[rows, 2 * WIDE :]
            j += 1


def local_parts(normed, stacks, fv, bound):
    seqs, heads, _, _, _ = fv.shape
    return pl.pallas_call(
        local_kernel,
        in_specs=[vmem_spec()] * (3 + len(stacks)),
        out_shape=pltpu.HBM((3, seqs // 2, heads, PAIR, HK), BF16),
        compiler_params=limit(14),
        name="local",
    )(normed, fv, bound, *stacks)


def out_weight(where, stacks, width):
    return pl.pallas_call(
        weight_kernel,
        in_specs=[pl.BlockSpec(memory_space=pltpu.SMEM)] + [vmem_spec()] * len(stacks),
        out_specs=vmem_spec(),
        out_shape=jax.ShapeDtypeStruct((WIDE, width), BF16),
        compiler_params=limit(4),
        name="weight",
    )(where, *stacks)


def output_kernel(state_ref, part_ref, fv_ref, weight_ref, norm_ref, post_ref, out_ref):
    heads = fv_ref.shape[1]
    pairs = out_ref.shape[0] // 2
    _, _, first_col = pair_masks()
    gain = norm_ref[...]
    rows = []
    for n_pair in range(pairs):
        p = n_pair
        gated = []
        for h in range(heads):
            runs, carried = [], []
            for n in range(2):
                s = pl.program_id(0) * 2 * pairs + 2 * p + n
                tail = state_ref[s, h, HV:, :].astype(F32)
                runs.append(tail[0:1, :] + tail[1:2, :] + tail[2:3, :])
                query = part_ref[0, p, h, n * CHUNK : (n + 1) * CHUNK, :]
                carried.append(dot_nt(query, state_ref[s, h, 0:HV, :]))
            run = jnp.where(first_col, runs[0], runs[1])
            run_cols = run.T
            weight = jnp.exp(jnp.minimum(run_cols - run, 0.0))
            scores = (part_ref[1, p, h].astype(F32) * weight).astype(BF16)
            v = fv_ref[2 * p : 2 * p + 2, h, 0].reshape(PAIR, HV)
            out = jnp.concatenate(carried, axis=0) * jnp.exp(run_cols) + dot(scores, v)
            scale = lax.rsqrt(jnp.mean(out * out, axis=-1, keepdims=True) + EPS)
            head = (out * scale * gain).astype(BF16).astype(F32)
            gate = part_ref[2, p, h].astype(F32)
            gated.append((head * (gate * sigmoid(gate))).astype(BF16))
        rows.append(jnp.concatenate(gated, axis=1))
    mixed = dot(jnp.concatenate(rows, axis=0), weight_ref[...])
    scale = lax.rsqrt(jnp.mean(mixed * mixed, axis=-1, keepdims=True) + EPS)
    out_ref[...] = (mixed * scale * post_ref[...]).astype(BF16).reshape(out_ref.shape)


def output_rows(states, parts, fv, weight, norm_gain, post_gain):
    seqs, heads, _, local_len, _ = fv.shape
    width = weight.shape[1]
    group = 4
    return pl.pallas_call(
        output_kernel,
        grid=(seqs // group,),
        in_specs=[
            vmem_spec(),
            pl.BlockSpec((3, group // 2, heads, PAIR, HK), lambda i: (0, i, 0, 0, 0)),
            pl.BlockSpec((group, heads, 1, local_len, HK), lambda i: (i, 0, 1, 0, 0)),
            vmem_spec(),
            vmem_spec(),
            vmem_spec(),
        ],
        out_specs=pl.BlockSpec((group, local_len, width), lambda i: (i, 0, 0)),
        out_shape=jax.ShapeDtypeStruct((seqs, local_len, width), BF16),
        compiler_params=limit(12),
        name="output",
    )(states, in_hbm(parts), in_hbm(fv), weight, norm_gain.reshape(1, HV), post_gain.reshape(1, width))


def layer(
    tokens,
    pre_gain,
    w_query,
    w_forget,
    w_value,
    w_gate,
    lower_bound,
    extra_decay,
    initial_state,
    norm_gain,
    w_out,
    post_gain,
):
    seqs, local_len, width = tokens.shape
    items = seqs * HEADS
    where = jnp.stack([lax.axis_index("y"), lax.axis_index("c")]).astype(jnp.int32)
    bound = lower_bound.reshape(1, HEADS * HK)
    head = lax.axis_index("x").astype(jnp.int32).reshape(1)

    first = joined((w_forget, w_value), ((0, (0, 0), (0, 0)), (1, (0, 0), (0, WIDE))), 2 * WIDE)
    places = [(0, (0, 0), (0, 0)), (1, (0, 0), (0, WIDE))]
    places += [(2, (0, n * WIDE), (n * OUT_ROWS, 2 * WIDE)) for n in range(width // WIDE)]
    second = joined((w_query, w_gate, w_out), tuple(places), 3 * WIDE)
    rows = tokens.reshape(seqs * local_len, width)
    normed = normed_tokens(rows, pre_gain, where)

    first_own, first_other = gathered_y(first, ((), (normed,), (second,), ()), True, 5)
    fv = project_heads(normed, first_own + first_other, seqs, local_len)
    moved = lax.all_to_all(fv.reshape(items, 2 * local_len, HK), SP, 0, 0, tiled=True)
    moved = moved.reshape(items, 2, local_len, HK)
    starts = chunk_states(moved, extra_decay, bound, initial_state, head)
    states = lax.all_to_all(starts, SP, 0, 0, tiled=True)

    second_own, second_other = gathered_y(second, ((), (), (), ()), False, 4)
    stacks = second_own + second_other
    parts = local_parts(normed, stacks, fv, bound)
    weight = out_weight(where, stacks, width)
    states = states.reshape(seqs, HEADS, HV + TAIL, HK)
    return output_rows(states, parts, fv, weight, norm_gain, post_gain)


def solution(mesh):
    split = Mesh(mesh.devices.reshape(8, 4, 8, 2), ("z", "x", "y", "c"))
    in_specs = (
        P(DP, SP, None),
        P(),
        P(DP, None),
        P(DP, None),
        P(DP, None),
        P(DP, None),
        P(),
        P(DP_SP, None),
        P(DP_SP, None, None),
        P(),
        P(DP, None),
        P(),
    )
    out_specs = P(DP, SP, None)
    return jax.shard_map(layer, mesh=split, in_specs=in_specs, out_specs=out_specs, check_vma=False)
```

```python
import functools

import jax
import jax.numpy as jnp
from jax import lax
from jax.experimental import pallas as pl
from jax.experimental.pallas import tpu as pltpu
from jax.sharding import Mesh
from jax.sharding import PartitionSpec as P


HEADS = 4
HK = 128
HV = 128
CHUNK = 64
PAIR = 2 * CHUNK
TAIL = 8
SP = ("z", "x")
DP = ("y", "c")
DP_SP = ("y", "c", "z", "x")
OFFSETS = (0, -1, 1, -2, 2, -3, 3, 4)
ROWS = 128
OUT_ROWS = 32
EPS = 1e-06
WIDE = HEADS * HV


F32 = jnp.float32
BF16 = jnp.bfloat16


def shifted(a, step):
    size = lax.axis_size("y")
    return lax.ppermute(a, "y", [(i, (i + step) % size) for i in range(size)])


def swapped(a):
    return lax.ppermute(a, "c", [(0, 1), (1, 0)])


def after(values, others):
    return lax.optimization_barrier((*values, *others))[: len(values)]


def gathered_y(shard, waits, halves, last):
    pieces = [shard]
    up = down = shard
    for k in range(4):
        up = after((up,), waits[k])[0] if waits[k] else up
        if k == 3 and halves:
            middle = shard.shape[0] // 2
            up, down = up[:middle], down[middle:]
        up = shifted(up, 1)
        if k < 3 or halves:
            down = shifted(down, -1)
        pieces += [up, down] if k < 3 or halves else [up]
    total = len(pieces)
    middle = total - last
    first = 5 if halves else 4
    own, other = [], []
    for part in (pieces[:first], pieces[first:middle], pieces[middle:]):
        if part:
            own.append(stacked_pieces(part) if len(part) > 1 else part[0])
            other.append(swapped(own[-1]))
    return own, other


def in_hbm(a):
    return pltpu.with_memory_space_constraint(a, pltpu.HBM)


def join_kernel(*refs, places):
    out_ref, sems = refs[-2:]
    copies = []
    for n, (k, (rows, cols), (r, c)) in enumerate(places):
        source = refs[k].at[:, pl.ds(cols, WIDE)]
        target = out_ref.at[pl.ds(r, source.shape[0]), pl.ds(c, WIDE)]
        copies.append(pltpu.make_async_copy(source, target, sems.at[n]))
    for copy in copies:
        copy.start()
    for copy in copies:
        copy.wait()


def joined(arrays, places, width):
    return pl.pallas_call(
        functools.partial(join_kernel, places=places),
        in_specs=[pl.BlockSpec(memory_space=pl.ANY)] * len(arrays),
        out_specs=vmem_spec(),
        out_shape=jax.ShapeDtypeStruct((ROWS, width), BF16),
        scratch_shapes=[pltpu.SemaphoreType.DMA((len(places),))],
        compiler_params=limit(2),
    )(*[in_hbm(a) for a in arrays])


def stack_kernel(*refs):
    out_ref = refs[-1]
    first = 0
    for ref in refs[:-1]:
        rows = ref.shape[0]
        out_ref[first : first + rows, :] = ref[...]
        first += rows


def stacked_pieces(pieces):
    rows = sum(p.shape[0] for p in pieces)
    return pl.pallas_call(
        stack_kernel,
        in_specs=[vmem_spec()] * len(pieces),
        out_specs=vmem_spec(),
        out_shape=jax.ShapeDtypeStruct((rows, pieces[0].shape[1]), BF16),
        compiler_params=limit(6),
        name="stack",
    )(*pieces)


def with_places(own, other):
    placed = []
    for k, parts in enumerate((own, other)):
        first = k * ROWS * len(OFFSETS)
        for part in parts:
            placed.append((first, part))
            first += part.shape[0]
    return placed


def against(a_ref, places, refs, cols):
    total = None
    for first, ref in zip(places, refs, strict=True):
        part = dot(a_ref[:, first : first + ref.shape[0]], ref[:, cols])
        total = part if total is None else total + part
    return total


def dot(a, b):
    return jnp.dot(a, b, preferred_element_type=F32)


def dot_nt(a, b):
    return lax.dot_general(a, b, (((1,), (1,)), ((), ())), preferred_element_type=F32)


def dot_tn(a, b):
    return lax.dot_general(a, b, (((0,), (0,)), ((), ())), preferred_element_type=F32)


def sigmoid(a):
    return 0.5 * jnp.tanh(0.5 * a) + 0.5


def place(where_ref, j):
    core = where_ref[1] if j < len(OFFSETS) else 1 - where_ref[1]
    return 2 * ((where_ref[0] + OFFSETS[j % len(OFFSETS)] + 8) & 7) + core


def norm_kernel(where_ref, x_ref, gain_ref, out_ref, held_ref, sems):
    tile = held_ref.shape[0] // sems.shape[0]
    copies = []
    for n in range(sems.shape[0]):
        rows = pl.ds(n * tile, tile)
        copies.append(pltpu.make_async_copy(x_ref.at[rows], held_ref.at[rows], sems.at[n]))
        copies[-1].start()
    for n, copy in enumerate(copies):
        copy.wait()
        rows = slice(n * tile, (n + 1) * tile)
        x = held_ref[rows, :].astype(F32)
        scale = lax.rsqrt(jnp.mean(x * x, axis=-1, keepdims=True) + EPS)
        for j in range(2 * len(OFFSETS)):
            cols = pl.ds(pl.multiple_of(place(where_ref, j) * ROWS, ROWS), ROWS)
            part = held_ref[rows, cols].astype(F32) * scale * gain_ref[:, cols]
            out_ref[rows, j * ROWS : (j + 1) * ROWS] = part.astype(BF16)


def normed_tokens(tokens, pre_gain, where):
    rows, width = tokens.shape
    return pl.pallas_call(
        norm_kernel,
        in_specs=[
            pl.BlockSpec(memory_space=pltpu.SMEM),
            pl.BlockSpec(memory_space=pl.ANY),
            vmem_spec(),
        ],
        out_specs=vmem_spec(),
        out_shape=jax.ShapeDtypeStruct((rows, width), BF16),
        scratch_shapes=[pltpu.VMEM((rows, width), BF16), pltpu.SemaphoreType.DMA((4,))],
        compiler_params=limit(6),
        name="norm",
    )(where, in_hbm(tokens), in_hbm(pre_gain.reshape(1, width)))


def vmem_spec():
    return pl.BlockSpec(memory_space=pltpu.VMEM)


def limit(mib):
    return pltpu.CompilerParams(vmem_limit_bytes=mib << 20)


def project_kernel(a_ref, *refs, places):
    out_ref = refs[-1]
    seqs, heads, _, local_len, _ = out_ref.shape
    wide = heads * HK
    cols = pl.ds(pl.multiple_of(pl.program_id(0) * wide, wide), wide)
    total = against(a_ref, places, refs[:-1], cols).astype(BF16)
    for n in range(heads):
        out_ref[:, n, 0] = total[:, n * HK : (n + 1) * HK].reshape(seqs, local_len, HK)


def project_heads(normed, placed, seqs, local_len):
    places, stacks = zip(*placed, strict=True)
    block = (seqs, 2, 1, local_len, HK)
    return pl.pallas_call(
        functools.partial(project_kernel, places=places),
        grid=(HEADS,),
        in_specs=[vmem_spec()] * (1 + len(stacks)),
        out_specs=pl.BlockSpec(block, lambda j: (0, j % 2, j // 2, 0, 0)),
        out_shape=pltpu.HBM((seqs, HEADS, 2, local_len, HK), BF16),
        compiler_params=limit(8),
        name="project",
    )(normed, *stacks)


def pair_masks():
    row = lax.broadcasted_iota(jnp.int32, (PAIR, PAIR), 0)
    col = lax.broadcasted_iota(jnp.int32, (PAIR, PAIR), 1)
    causal = (row >= col) & ((row < CHUNK) == (col < CHUNK))
    return causal, row < CHUNK, col < CHUNK


def keys_and_total(f, gap, ones):
    keys = gap * sigmoid(-f)
    decay = jnp.log1p(-keys)
    high = decay.astype(BF16)
    low = (decay - high.astype(F32)).astype(BF16)
    return keys, dot(ones, high) + dot(ones, low)


def parts_of(a):
    high = a.astype(BF16).astype(F32)
    middle = (a - high).astype(BF16).astype(F32)
    return high, middle, a - high - middle


def state_kernel(head_ref, fv_ref, extra_ref, bound_ref, state_ref, out_ref, carry_ref, run_ref):
    chunks = out_ref.shape[0]
    causal, first_row, first_col = pair_masks()
    ones = causal.astype(F32).astype(BF16)
    gap = 1.0 - bound_ref[:, pl.ds(pl.multiple_of(head_ref[0] * HK, HK), HK)]
    tail_row = lax.broadcasted_iota(jnp.int32, (TAIL, HK), 0)
    block = pl.program_id(0)

    @pl.when(block == 0)
    def _():
        carry_ref[...] = state_ref[0].T
        for p in range(run_ref.shape[0]):
            run_ref[p : p + 1, :] = extra_ref[:, p * PAIR : (p + 1) * PAIR]
        split = [part.astype(BF16) for part in parts_of(run_ref[...])]
        run_ref[...] = sum(dot_nt(part, ones) for part in split)

    state = carry_ref[...]
    for p in range(chunks // 2):
        b = block * chunks + 2 * p
        f = fv_ref[pl.ds(b, 2), 0].reshape(PAIR, HK).astype(F32)
        keys, total = keys_and_total(f, gap, ones)
        run_row = run_ref[pl.ds(block * (chunks // 2) + p, 1), :]
        run = jnp.broadcast_to(run_row, (PAIR, PAIR)).T
        ends = [total[n * CHUNK + CHUNK - 1 : (n + 1) * CHUNK, :] for n in range(2)]
        run_ends = [run[n * CHUNK + CHUNK - 1 : (n + 1) * CHUNK, :] for n in range(2)]
        end = jnp.where(first_row, ends[0], ends[1])
        run_end = jnp.where(first_row, run_ends[0], run_ends[1])
        weighted = (keys * jnp.exp((end - total) + (run_end - run))).astype(BF16)
        own = jnp.broadcast_to(run_row, (TAIL, PAIR))
        turned = pltpu.roll(own, CHUNK, 1)
        first_lane = first_col[0:TAIL, :]
        for n in range(2):
            both = jnp.where(first_lane, own, turned) if n == 0 else jnp.where(first_lane, turned, own)
            high, middle, low = parts_of(both)
            tail = jnp.where(tail_row == 0, high, jnp.where(tail_row == 1, middle, low))
            out_ref[2 * p + n, 0:HV, :] = state.astype(BF16)
            out_ref[2 * p + n, HV:, :] = tail.astype(BF16)
            rows = slice(n * CHUNK, (n + 1) * CHUNK)
            added = dot_tn(fv_ref[b + n, 1], weighted[rows])
            state = state * jnp.exp(ends[n] + run_ends[n]) + added
    carry_ref[...] = state


def chunk_states(fv, extra, bound, state, head):
    chunks = fv.shape[0]
    group = 8
    return pl.pallas_call(
        state_kernel,
        grid=(chunks // group,),
        in_specs=[
            pl.BlockSpec(memory_space=pltpu.SMEM),
            vmem_spec(),
            pl.BlockSpec(extra.shape, lambda i: (0, 0)),
            pl.BlockSpec(bound.shape, lambda i: (0, 0)),
            pl.BlockSpec(state.shape, lambda i: (0, 0, 0)),
        ],
        out_specs=pl.BlockSpec((group, HV + TAIL, HK), lambda i: (i, 0, 0)),
        out_shape=pltpu.HBM((chunks, HV + TAIL, HK), BF16),
        scratch_shapes=[pltpu.VMEM((HV, HK), F32), pltpu.VMEM((chunks // 2, PAIR), F32)],
        compiler_params=limit(6),
        name="state",
    )(head, fv, in_hbm(extra), in_hbm(bound), in_hbm(state))


def begun_kernel(a_ref, fv_ref, bound_ref, *refs, places):
    out_ref, stacks = refs[-1], refs[:-1]
    seqs, heads, _, _, _ = fv_ref.shape
    causal, _, _ = pair_masks()
    ones = causal.astype(F32).astype(BF16)
    out_ref[:, : 2 * WIDE] = against(a_ref, places, stacks, slice(0, 2 * WIDE))
    for p in range(seqs // 2):
        rows = slice(p * PAIR, (p + 1) * PAIR)
        for h in range(heads):
            f = fv_ref[2 * p : 2 * p + 2, h, 0].reshape(PAIR, HK).astype(F32)
            keys, total = keys_and_total(f, 1.0 - bound_ref[:, h * HK : (h + 1) * HK], ones)
            first = 2 * WIDE + h * HK
            out_ref[rows, first : first + HK] = jnp.exp(total)
            out_ref[rows, first + WIDE : first + WIDE + HK] = keys * jnp.exp(-total)


def begun_parts(normed, placed, fv, bound):
    places, stacks = zip(*placed, strict=True)
    return pl.pallas_call(
        functools.partial(begun_kernel, places=places),
        in_specs=[vmem_spec()] * (3 + len(stacks)),
        out_specs=vmem_spec(),
        out_shape=jax.ShapeDtypeStruct((normed.shape[0], 4 * WIDE), F32),
        compiler_params=limit(14),
        name="begun",
    )(normed, fv, bound, *stacks)


def local_kernel(a_ref, begun_ref, *refs, places):
    out_ref, stacks = refs[-1], refs[:-1]
    _, pairs, heads, _, _ = out_ref.shape
    causal, _, _ = pair_masks()
    rest = against(a_ref, places, stacks, slice(0, 2 * WIDE))
    pre = (begun_ref[:, : 2 * WIDE] + rest).astype(BF16)
    for p in range(pairs):
        rows = slice(p * PAIR, (p + 1) * PAIR)
        for h in range(heads):
            cols = slice(h * HK, (h + 1) * HK)
            q = pre[rows, cols].astype(F32)
            first = 2 * WIDE + h * HK
            decay = begun_ref[rows, first : first + HK]
            k_scaled = begun_ref[rows, first + WIDE : first + WIDE + HK].astype(BF16)
            q_scaled = (q * sigmoid(q) * decay).astype(BF16)
            out_ref[0, p, h] = q_scaled
            out_ref[1, p, h] = jnp.where(causal, dot_nt(q_scaled, k_scaled), 0.0).astype(BF16)
            out_ref[2, p, h] = pre[rows, WIDE + h * HV : WIDE + (h + 1) * HV]


def weight_kernel(where_ref, *refs):
    weight_ref = refs[-1]
    j = 0
    for stack in refs[:-1]:
        for first in range(0, stack.shape[0], ROWS):
            start = pl.multiple_of(place(where_ref, j) * OUT_ROWS, OUT_ROWS)
            for n in range(ROWS // OUT_ROWS):
                rows = slice(first + n * OUT_ROWS, first + (n + 1) * OUT_ROWS)
                weight_ref[pl.ds(start, OUT_ROWS), n * WIDE : (n + 1) * WIDE] = stack[rows, 2 * WIDE :]
            j += 1


def local_parts(normed, placed, begun):
    places, stacks = zip(*placed, strict=True)
    pairs = normed.shape[0] // PAIR
    return pl.pallas_call(
        functools.partial(local_kernel, places=places),
        in_specs=[vmem_spec()] * (2 + len(stacks)),
        out_shape=pltpu.HBM((3, pairs, HEADS, PAIR, HK), BF16),
        compiler_params=limit(14),
        name="local",
    )(normed, begun, *stacks)


def out_weight(where, stacks, width):
    return pl.pallas_call(
        weight_kernel,
        in_specs=[pl.BlockSpec(memory_space=pltpu.SMEM)] + [vmem_spec()] * len(stacks),
        out_specs=vmem_spec(),
        out_shape=jax.ShapeDtypeStruct((WIDE, width), BF16),
        compiler_params=limit(4),
        name="weight",
    )(where, *stacks)


def output_kernel(state_ref, part_ref, fv_ref, weight_ref, norm_ref, post_ref, out_ref):
    heads = fv_ref.shape[1]
    pairs = out_ref.shape[0] // 2
    _, _, first_col = pair_masks()
    gain = norm_ref[...]
    rows = []
    for n_pair in range(pairs):
        p = n_pair
        gated = []
        for h in range(heads):
            runs, carried = [], []
            for n in range(2):
                s = pl.program_id(0) * 2 * pairs + 2 * p + n
                tail = state_ref[s, h, HV:, :].astype(F32)
                runs.append(tail[0:1, :] + tail[1:2, :] + tail[2:3, :])
                query = part_ref[0, p, h, n * CHUNK : (n + 1) * CHUNK, :]
                carried.append(dot_nt(query, state_ref[s, h, 0:HV, :]))
            run = jnp.where(first_col, runs[0], runs[1])
            run_cols = run.T
            weight = jnp.exp(jnp.minimum(run_cols - run, 0.0))
            scores = (part_ref[1, p, h].astype(F32) * weight).astype(BF16)
            v = fv_ref[2 * p : 2 * p + 2, h, 0].reshape(PAIR, HV)
            out = jnp.concatenate(carried, axis=0) * jnp.exp(run_cols) + dot(scores, v)
            scale = lax.rsqrt(jnp.mean(out * out, axis=-1, keepdims=True) + EPS)
            head = (out * scale * gain).astype(BF16).astype(F32)
            gate = part_ref[2, p, h].astype(F32)
            gated.append((head * (gate * sigmoid(gate))).astype(BF16))
        rows.append(jnp.concatenate(gated, axis=1))
    mixed = dot(jnp.concatenate(rows, axis=0), weight_ref[...])
    scale = lax.rsqrt(jnp.mean(mixed * mixed, axis=-1, keepdims=True) + EPS)
    out_ref[...] = (mixed * scale * post_ref[...]).astype(BF16).reshape(out_ref.shape)


def output_rows(states, parts, fv, weight, norm_gain, post_gain):
    seqs, heads, _, local_len, _ = fv.shape
    width = weight.shape[1]
    group = 4
    return pl.pallas_call(
        output_kernel,
        grid=(seqs // group,),
        in_specs=[
            vmem_spec(),
            pl.BlockSpec((3, group // 2, heads, PAIR, HK), lambda i: (0, i, 0, 0, 0)),
            pl.BlockSpec((group, heads, 1, local_len, HK), lambda i: (i, 0, 1, 0, 0)),
            vmem_spec(),
            vmem_spec(),
            vmem_spec(),
        ],
        out_specs=pl.BlockSpec((group, local_len, width), lambda i: (i, 0, 0)),
        out_shape=jax.ShapeDtypeStruct((seqs, local_len, width), BF16),
        compiler_params=limit(12),
        name="output",
    )(states, in_hbm(parts), in_hbm(fv), weight, norm_gain.reshape(1, HV), post_gain.reshape(1, width))


def layer(
    tokens,
    pre_gain,
    w_query,
    w_forget,
    w_value,
    w_gate,
    lower_bound,
    extra_decay,
    initial_state,
    norm_gain,
    w_out,
    post_gain,
):
    seqs, local_len, width = tokens.shape
    items = seqs * HEADS
    where = jnp.stack([lax.axis_index("y"), lax.axis_index("c")]).astype(jnp.int32)
    bound = lower_bound.reshape(1, HEADS * HK)
    head = lax.axis_index("x").astype(jnp.int32).reshape(1)

    first = joined((w_forget, w_value), ((0, (0, 0), (0, 0)), (1, (0, 0), (0, WIDE))), 2 * WIDE)
    places = [(0, (0, 0), (0, 0)), (1, (0, 0), (0, WIDE))]
    places += [(2, (0, n * WIDE), (n * OUT_ROWS, 2 * WIDE)) for n in range(width // WIDE)]
    second = joined((w_query, w_gate, w_out), tuple(places), 3 * WIDE)
    rows = tokens.reshape(seqs * local_len, width)
    normed = normed_tokens(rows, pre_gain, where)

    first_own, first_other = gathered_y(first, ((), (normed,), (second,), ()), True, 4)
    fv = project_heads(normed, with_places(first_own, first_other), seqs, local_len)
    moved = lax.all_to_all(fv.reshape(items, 2 * local_len, HK), SP, 0, 0, tiled=True)
    moved = moved.reshape(items, 2, local_len, HK)
    starts = chunk_states(moved, extra_decay, bound, initial_state, head)
    states = lax.all_to_all(starts, SP, 0, 0, tiled=True)

    second_own, second_other = gathered_y(second, ((), (), (), ()), False, 2)
    stacks = second_own + second_other
    placed = with_places(second_own, second_other)
    cut = len(second_own)
    begun = begun_parts(normed, [placed[0], placed[cut]], fv, bound)
    parts = local_parts(normed, placed[1:cut] + placed[cut + 1 :], begun)
    weight = out_weight(where, stacks, width)
    states = states.reshape(seqs, HEADS, HV + TAIL, HK)
    return output_rows(states, parts, fv, weight, norm_gain, post_gain)


def solution(mesh):
    split = Mesh(mesh.devices.reshape(8, 4, 8, 2), ("z", "x", "y", "c"))
    in_specs = (
        P(DP, SP, None),
        P(),
        P(DP, None),
        P(DP, None),
        P(DP, None),
        P(DP, None),
        P(),
        P(DP_SP, None),
        P(DP_SP, None, None),
        P(),
        P(DP, None),
        P(),
    )
    out_specs = P(DP, SP, None)
    return jax.shard_map(layer, mesh=split, in_specs=in_specs, out_specs=out_specs, check_vma=False)
```
